32 devices in a mesh: fs: 4 (over z), rep: 4 (over y, x), tp: 2 (over core).
Axes of the slice: x: 2, y: 2, z: 4, core: 2. Of those that a mesh axis runs over, the one named last changes fastest.
Arguments:
- inputs: bfloat16 [2048, 2048], P(('fs', 'rep')), may hold values from -6 to 6
- query_cot: bfloat16 [2048, 1024], P(('fs', 'rep'), 'tp'), may hold values from -0.125 to 0.125
- attended: bfloat16 [2048, 1024], P(('fs', 'rep')), may hold values from -6 to 6
- output_cot: bfloat16 [2048, 2048], P(('fs', 'rep'), 'tp'), may hold values from -0.125 to 0.125
- proj_query: bfloat16 [2048, 256], P('fs'), may hold values from -0.125 to 0.125
- proj_output: bfloat16 [1024, 256], P('fs'), may hold values from -0.1875 to 0.1875
- weight_query: float32 [2048, 1024], P('fs', 'tp'), may hold values from -0.125 to 0.125
- weight_output: float32 [1024, 2048], P('fs', 'tp'), may hold values from -0.1875 to 0.1875
- first_query: float32 [256, 1024], P('fs', 'tp'), may hold values from -6 to 6
- second_query: float32 [256, 1024], P('fs', 'tp'), may hold values from 0.0002 to 2
- first_output: float32 [256, 2048], P('fs', 'tp'), may hold values from -6 to 6
- second_output: float32 [256, 2048], P('fs', 'tp'), may hold values from 0.0002 to 2
Outputs:
- new_weight_query: float32 [2048, 1024], P('fs', 'tp')
- new_weight_output: float32 [1024, 2048], P('fs', 'tp')
- step_query: float32 [2048, 1024], P('fs', 'tp')
- step_output: float32 [1024, 2048], P('fs', 'tp')
- new_first_query: float32 [256, 1024], P('fs', 'tp')
- new_second_query: float32 [256, 1024], P('fs', 'tp')
- new_first_output: float32 [256, 2048], P('fs', 'tp')
- new_second_output: float32 [256, 2048], P('fs', 'tp')
- copy_query: bfloat16 [2048, 1024], P(None, 'tp')
- copy_output: bfloat16 [1024, 2048], P(None, 'tp')
The draws below stay inside these ranges and needn't reach their ends.
All inputs are finite; a program needn't handle non-finite values.
Results may differ from the reference program's by a relative error of at most 0.0031.
Values may be sent and summed in bfloat16 or wider, within the bound.
No kernel may reach another device: no remote copies, remote signals or barrier semaphores. Data moves between devices by JAX's collectives and lax.ppermute only.
A program may use at most 64 MiB of HBM per device.

```python
import jax
import jax.numpy as jnp
from jax import lax

D = 2048
DA = 1024
RANK = 256
TOKENS = 2048


def variance_table(key, height, breadth):
    base = jnp.exp(jax.random.uniform(key, (height, breadth), jnp.float32, jnp.log(0.02), jnp.log(1.0)))
    row_place = jnp.arange(height, dtype=jnp.float32) / height
    col_place = jnp.arange(breadth, dtype=jnp.float32) / breadth
    return base * jnp.exp(-jnp.log(10.0) * row_place)[:, None] * jnp.exp(-jnp.log(10.0) * col_place)[None, :]


def draw_second_query(key, part):
    return variance_table(jax.random.fold_in(key, 11), RANK, DA)


def draw_second_output(key, part):
    return variance_table(jax.random.fold_in(key, 12), RANK, D)


def with_spikes(drawn, stream_key, source, target, parts, factor):
    owner, partner = [(jnp.arange(drawn.shape[axis_at]) // (drawn.shape[axis_at] // parts)).reshape([-1 if axis == axis_at else 1 for axis in range(drawn.ndim)]) for axis_at in (source, target)]
    chosen = jax.random.permutation(stream_key, parts)[partner]
    strong = (owner == chosen) | (owner == (partner + parts // 2) % parts)
    return jnp.where(strong, factor * drawn, drawn)


def block_scale(own_key, extent, cuts, least, top_value):
    factor_of = 1.0
    for axis_at, shards_of in cuts:
        draws = jax.random.uniform(jax.random.fold_in(jax.random.fold_in(own_key, 6), axis_at), (shards_of,), jnp.float32, least / len(cuts), top_value / len(cuts))
        factor_of = factor_of * jnp.repeat(jnp.exp(draws), extent[axis_at] // shards_of).reshape((-1,) + (1,) * (len(extent) - 1 - axis_at))
    return factor_of


def scatter_about(rng, extent, scale, most, pieces=(), kind=jnp.bfloat16):
    values = scale * jax.random.normal(rng, extent, jnp.float32)
    if pieces:
        values = values * block_scale(rng, extent, pieces, -0.22, 0.18)
    return jnp.clip(values, -most, most).astype(kind)


def bell_draw_with(key, shape, scale, reach, pieces, heavy, kind=jnp.bfloat16):
    values = scale * jax.random.normal(key, shape, jnp.float32)
    if pieces:
        values = values * block_scale(key, shape, pieces, -0.22, 0.18)
    return jnp.clip(with_spikes(values, jax.random.fold_in(key, 3), *heavy), -reach, reach).astype(kind)


def setup_inputs(seed: int = 0) -> dict:
    keys = jax.random.split(jax.random.key(seed), 13)
    inputs = bell_draw_with(keys[0], (TOKENS, D), 1.0, 6.0, ((0, 16),), (0, 1, 16, 2.0))
    query_cot = scatter_about(keys[1], (TOKENS, DA), TOKENS ** -0.5, 0.125, ((0, 16), (1, 2)))
    attended = bell_draw_with(keys[2], (TOKENS, DA), 1.0, 6.0, ((0, 16),), (0, 1, 16, 2.0))
    output_cot = scatter_about(keys[3], (TOKENS, D), TOKENS ** -0.5, 0.125, ((0, 16), (1, 2)))
    proj_query = scatter_about(keys[4], (D, RANK), D ** -0.5, 0.125, ((0, 4),))
    proj_output = scatter_about(keys[5], (DA, RANK), DA ** -0.5, 0.1875, ((0, 4),))
    weight_query = scatter_about(keys[6], (D, DA), D ** -0.5, 0.125, ((0, 4), (1, 2)), jnp.float32)
    weight_output = scatter_about(keys[7], (DA, D), DA ** -0.5, 0.1875, ((0, 4), (1, 2)), jnp.float32)
    first_query = scatter_about(keys[8], (RANK, DA), 1.0, 6.0, ((0, 4), (1, 2)), jnp.float32)
    second_query = draw_second_query(jax.random.fold_in(keys[12], 71), 0)
    first_output = scatter_about(keys[10], (RANK, D), 1.0, 6.0, ((0, 4), (1, 2)), jnp.float32)
    second_output = draw_second_output(jax.random.fold_in(keys[12], 71), 0)
    return dict(inputs=inputs, query_cot=query_cot, attended=attended, output_cot=output_cot, proj_query=proj_query, proj_output=proj_output, weight_query=weight_query, weight_output=weight_output, first_query=first_query, second_query=second_query, first_output=first_output, second_output=second_output)


beta_first = 0.9
beta_second = 0.95
adam_eps = 1e-08
mean_eps = 1e-06
learn_rate = 0.02

def contract_rows(left, right, high):
    if high:
        return lax.dot_general(left, right, (((0,), (0,)), ((), ())), precision=lax.Precision.HIGHEST, preferred_element_type=jnp.float32)
    return lax.dot_general(left, right, (((0,), (0,)), ((), ())), preferred_element_type=jnp.float32)

def moment_update(low_sum, first, second):
    first_new = beta_first * first + (1.0 - beta_first) * low_sum
    second_new = beta_second * second + (1.0 - beta_second) * low_sum * low_sum
    normed = first_new / (jnp.sqrt(second_new) + adam_eps)
    return (first_new, second_new, normed)

def reference(inputs, query_cot, attended, output_cot, proj_query, proj_output, weight_query, weight_output, first_query, second_query, first_output, second_output):
    grad_query = contract_rows(inputs, query_cot, False)
    grad_output = contract_rows(attended, output_cot, False)
    low_query = contract_rows(proj_query.astype(jnp.float32), grad_query, True)
    low_output = contract_rows(proj_output.astype(jnp.float32), grad_output, True)
    first_q, second_q, normed_q = moment_update(low_query, first_query, second_query)
    first_o, second_o, normed_o = moment_update(low_output, first_output, second_output)
    entries = RANK * (DA + D)
    total = jnp.sum(normed_q * normed_q) + jnp.sum(normed_o * normed_o)
    scale = lax.rsqrt(total / entries + mean_eps)
    half_q = normed_q.astype(jnp.bfloat16)
    half_o = normed_o.astype(jnp.bfloat16)
    step_q = scale * jnp.dot(proj_query, half_q, preferred_element_type=jnp.float32)
    step_o = scale * jnp.dot(proj_output, half_o, preferred_element_type=jnp.float32)
    new_q = weight_query - learn_rate * step_q
    new_o = weight_output - learn_rate * step_o
    return (new_q, new_o, step_q, step_o, first_q, second_q, first_o, second_o, new_q.astype(jnp.bfloat16), new_o.astype(jnp.bfloat16))
```

```python
import jax
import jax.numpy as jnp
from jax import lax
from jax.experimental import pallas as pl
from jax.experimental.pallas import tpu as pltpu
from jax.sharding import PartitionSpec as P

beta_first = 0.9
beta_second = 0.95
adam_eps = 1e-08
mean_eps = 1e-06
learn_rate = 0.02
code_scale = 2.0**17


f32 = jnp.float32
bf16 = jnp.bfloat16
VMEM = pl.BlockSpec(memory_space=pltpu.VMEM)
SMEM = pl.BlockSpec(memory_space=pltpu.SMEM)
TAIL = 16


def moment_update(low_sum, first, second):
    first_new = beta_first * first + (1.0 - beta_first) * low_sum
    second_new = beta_second * second + (1.0 - beta_second) * low_sum * low_sum
    normed = first_new / (jnp.sqrt(second_new) + adam_eps)
    return (first_new, second_new, normed)


def contract_rows(left, right):
    return lax.dot_general(
        left,
        right,
        (((0,), (0,)), ((), ())),
        precision=lax.Precision.HIGHEST,
        preferred_element_type=f32,
    )


def local_general(inputs, query_cot, attended, output_cot, proj_query, proj_output, weight_query, weight_output, first_query, second_query, first_output, second_output):
    def gather(x):
        return lax.all_gather(x, "fs", axis=0, tiled=True)

    def low_of(acts, proj, cot):
        reduced = jnp.dot(acts, gather(proj), preferred_element_type=f32)
        part = contract_rows(reduced, cot.astype(f32))
        return lax.psum_scatter(part, "fs", scatter_dimension=0, tiled=True)

    low_query, low_output = lax.psum((low_of(inputs, proj_query, query_cot), low_of(attended, proj_output, output_cot)), "rep")
    first_q, second_q, normed_q = moment_update(low_query, first_query, second_query)
    first_o, second_o, normed_o = moment_update(low_output, first_output, second_output)
    total = lax.psum(jnp.sum(normed_q * normed_q) + jnp.sum(normed_o * normed_o), ("fs", "tp"))
    entries = (normed_q.size + normed_o.size) * lax.axis_size("fs") * lax.axis_size("tp")
    scale = lax.rsqrt(total / entries + mean_eps)
    step_q = scale * jnp.dot(proj_query, gather(normed_q.astype(bf16)), preferred_element_type=f32)
    step_o = scale * jnp.dot(proj_output, gather(normed_o.astype(bf16)), preferred_element_type=f32)
    new_q = weight_query - learn_rate * step_q
    new_o = weight_output - learn_rate * step_o
    return (new_q, new_o, step_q, step_o, first_q, second_q, first_o, second_o, gather(new_q.astype(bf16)), gather(new_o.astype(bf16)))


def reduce_kernel(nf, nr, place, inputs, attended, proj_q, proj_o, own, *rest):
    near, (all_q, all_o, red) = rest[:-3], rest[-3:]
    f, r, t = place[0], place[1], place[2]
    rows_q, half = proj_q.shape[0], all_q.shape[1]
    rows_o = proj_o.shape[0]
    part_q, part_o = rows_q // nr, rows_o // nr
    part = part_q + part_o
    mine = pl.ds(pl.multiple_of(t * half, half), half)
    all_q[pl.ds(pl.multiple_of(f * rows_q, rows_q), rows_q), :] = proj_q[:, mine]
    all_o[pl.ds(pl.multiple_of(f * rows_o, rows_o), rows_o), :] = proj_o[:, mine]
    for mr, ref in enumerate((own,) + near):
        for mz in range(1, nf):
            at = (f ^ mz) * nr + (r ^ mr)
            base = (mz - 1) * part
            all_q[pl.ds(pl.multiple_of(at * part_q, part_q), part_q), :] = ref[base : base + part_q, :]
            all_o[pl.ds(pl.multiple_of(at * part_o, part_o), part_o), :] = ref[base + part_q : base + part, :]
    red_q = jnp.dot(inputs[...], all_q[...], preferred_element_type=f32)
    red_o = jnp.dot(attended[...], all_o[...], preferred_element_type=f32)
    red[0:half, :] = red_q.T
    red[half : 2 * half, :] = red_o.T


def split_three(x):
    high = x.astype(bf16)
    rest = x - high.astype(f32)
    mid = rest.astype(bf16)
    return high, mid, (rest - mid.astype(f32)).astype(bf16)


def low_kernel(nf, nr, block_q, place, *refs):
    cots, mine, other, outs, low = refs[:nr], refs[nr : 2 * nr], refs[2 * nr : 3 * nr], refs[3 * nr : 3 * nr + nf], refs[-1]
    f, t = place[0], place[2]
    half = mine[0].shape[0] // 2
    cot = jnp.concatenate([c[...] for c in cots], axis=0)
    for which, group in enumerate((mine, other)):
        top = pl.multiple_of((t ^ which) * half, half)
        for k, (lo, hi) in enumerate(((0, block_q), (block_q, cot.shape[1]))):
            left = jnp.concatenate([g[k * half : (k + 1) * half, :] for g in group], axis=1)
            acc = None
            for term in split_three(left):
                got = jnp.dot(term, cot[:, lo:hi], preferred_element_type=f32)
                acc = got if acc is None else acc + got
            low[pl.ds(top, half), lo:hi] = acc
    rows = low.shape[0] // nf
    for m in range(nf):
        outs[m][...] = low[pl.ds(pl.multiple_of((f ^ m) * rows, rows), rows), :]


def moment_kernel(nf, block_q, place, *refs):
    parts, (first_q, second_q, first_o, second_o, low_out, half_out) = refs[:nf], refs[nf:]
    r = place[1]
    low = parts[0][...]
    for p in parts[1:]:
        low = low + p[...]
    low_out[...] = low
    block_o = low.shape[1] - block_q
    rows = low.shape[0]
    total = jnp.zeros((), f32)
    for first, second, lo, width in ((first_q, second_q, 0, block_q), (first_o, second_o, block_q, block_o)):
        cols = pl.ds(pl.multiple_of(r * width, width), width)
        _, _, normed = moment_update(low[:, lo : lo + width], first[:, cols], second[:, cols])
        half_out[0:rows, lo : lo + width] = normed.astype(bf16)
        total = total + jnp.sum(normed * normed)
    spread = jnp.full((8, low.shape[1]), total, f32)
    row = lax.broadcasted_iota(jnp.int32, spread.shape, 0)
    high, mid, last = (x.astype(f32) for x in split_three(spread))
    packed = jnp.where(row == 0, high, jnp.where(row == 1, mid, jnp.where(row == 2, last, 0.0)))
    half_out[rows : rows + TAIL, :] = jnp.concatenate([packed, jnp.zeros_like(packed)], axis=0).astype(bf16)


def state_kernel(nr, block_q, place, *refs):
    lows, (first_q, second_q, first_o, second_o, new_fq, new_sq, new_fo, new_so) = refs[:nr], refs[nr:]
    r = place[1]
    for m in range(nr):
        low = lows[m][...]
        block_o = low.shape[1] - block_q
        for first, second, new_f, new_s, lo, width in (
            (first_q, second_q, new_fq, new_sq, 0, block_q),
            (first_o, second_o, new_fo, new_so, block_q, block_o),
        ):
            cols = pl.ds(pl.multiple_of((r ^ m) * width, width), width)
            first_new, second_new, _ = moment_update(low[:, lo : lo + width], first[:, cols], second[:, cols])
            new_f[:, cols] = first_new
            new_s[:, cols] = second_new


def step_kernel(nf, nr, block_q, place, scale, own_q, own_o, oth_q, oth_o, *rest):
    halves, (codes, weight_q, weight_o, copy_q, copy_o, new_q, new_o, step_q, step_o, table_q, table_o) = rest[:nr], rest[nr:]
    f, r, t = place[0], place[1], place[2]
    mr, mz = pl.program_id(0), pl.program_id(1)
    half = own_q.shape[1]
    rank, cols_q = table_q.shape
    cols_o = table_o.shape[1]
    block_o = halves[0].shape[1] - block_q
    rows = rank // nf

    @pl.when(jnp.logical_and(mr == 0, mz == 0))
    def _():
        for m in range(nr):
            for z in range(nf):
                at = (f ^ z) * rows
                top = ((at // half) ^ t) * half + at % half
                to = pl.ds(pl.multiple_of(top, rows), rows)
                base = z * (rows + TAIL)
                table_q[to, pl.ds(pl.multiple_of((r ^ m) * block_q, block_q), block_q)] = halves[m][base : base + rows, 0:block_q]
                table_o[to, pl.ds(pl.multiple_of((r ^ m) * block_o, block_o), block_o)] = halves[m][base : base + rows, block_q:]

    part_q, part_o = weight_q.shape[0], weight_o.shape[0]
    at = (f ^ mz) * nr + (r ^ mr)
    from_q = pl.ds(pl.multiple_of(at * part_q, part_q), part_q)
    from_o = pl.ds(pl.multiple_of(at * part_o, part_o), part_o)
    left_q = jnp.concatenate([own_q[from_q, :], oth_q[from_q, :]], axis=1)
    left_o = jnp.concatenate([own_o[from_o, :], oth_o[from_o, :]], axis=1)
    got_q = scale[0] * jnp.dot(left_q, table_q[...], preferred_element_type=f32)
    got_o = scale[0] * jnp.dot(left_o, table_o[...], preferred_element_type=f32)

    @pl.when(mz == 0)
    def _():
        fresh_q = weight_q[...] - learn_rate * got_q
        fresh_o = weight_o[...] - learn_rate * got_o
        step_q[...] = got_q
        step_o[...] = got_o
        new_q[...] = fresh_q
        new_o[...] = fresh_o
        copy_q[...] = fresh_q.astype(bf16)
        copy_o[...] = fresh_o.astype(bf16)

    @pl.when(mz != 0)
    def _():
        code = codes[0, 0]
        copy_q[...] = (code[0:part_q, :] - learn_rate * got_q).astype(bf16)
        for k in range(cols_o // cols_q):
            old = code[part_q + k * part_o : part_q + (k + 1) * part_o, :]
            lo = k * cols_q
            copy_o[:, lo : lo + cols_q] = (old - learn_rate * got_o[:, lo : lo + cols_q]).astype(bf16)


def shape(x, dtype=f32):
    return jax.ShapeDtypeStruct(tuple(x), dtype)


def call(kernel, name, outs, scratch=(), cost=None):
    def run(place, *args):
        return pl.pallas_call(
            kernel,
            out_shape=outs,
            in_specs=[SMEM] + [VMEM] * len(args),
            out_specs=[VMEM] * len(outs),
            scratch_shapes=scratch,
            name=name,
            cost_estimate=cost,
        )(place, *args)

    return run


def local_short(nf, nr, inputs, query_cot, attended, output_cot, proj_query, proj_output, weight_query, weight_output, first_query, second_query, first_output, second_output):
    f, r, t = (lax.axis_index(a) for a in ("fs", "rep", "tp"))
    place = jnp.stack([f, r, t]).astype(jnp.int32)

    def swap(x, axis, m, n):
        return lax.ppermute(x, axis, [(i, i ^ m) for i in range(n)])

    def over_fs(x, m):
        return swap(x, "fs", m, nf)

    def over_rep(x, m):
        return swap(x, "rep", m, nr)

    def over_tp(x):
        return swap(x, "tp", 1, 2)

    tokens = inputs.shape[0]
    rank = proj_query.shape[1]
    half = rank // 2
    rows_q, rows_o = proj_query.shape[0], proj_output.shape[0]
    part_q, part_o = rows_q // nr, rows_o // nr
    cols_q, cols_o = query_cot.shape[1], output_cot.shape[1]
    block_q, block_o = cols_q // nr, cols_o // nr
    block = block_q + block_o
    rows = rank // nf
    fs_order = list(range(nf - 1, 0, -1))
    rep_order = list(range(nr - 1, 0, -1))

    share = jnp.concatenate(
        [
            lax.dynamic_slice(proj_query, (r * part_q, t * half), (part_q, half)),
            lax.dynamic_slice(proj_output, (r * part_o, t * half), (part_o, half)),
        ],
        axis=0,
    )
    far = {m: over_fs(share, m) for m in fs_order}

    def cot_block(which):
        return jnp.concatenate(
            [
                lax.dynamic_slice(query_cot, (0, which * block_q), (tokens, block_q)),
                lax.dynamic_slice(output_cot, (0, which * block_o), (tokens, block_o)),
            ],
            axis=1,
        )

    cots = {m: over_rep(cot_block(r ^ m), m) for m in rep_order}
    cots[0] = cot_block(r)

    own = jnp.concatenate([far[m] for m in range(1, nf)], axis=0)
    near = {m: over_rep(own, m) for m in rep_order}

    code = jnp.concatenate(
        [lax.dynamic_slice(weight_query, (r * part_q, 0), (part_q, cols_q))]
        + [lax.dynamic_slice(weight_output, (r * part_o, k * cols_q), (part_o, cols_q)) for k in range(cols_o // cols_q)],
        axis=0,
    )
    code = (code * code_scale).astype(jnp.float16)
    code_far = {m: over_fs(code, m) for m in fs_order}
    code_own = jnp.stack([code_far[m] for m in range(1, nf)])
    codes = {m: over_rep(code_own, m) for m in rep_order}
    codes[0] = code_own

    all_q, all_o, red = call(
        lambda *a: reduce_kernel(nf, nr, *a),
        "reduce",
        [shape((rows_q * nf, half), bf16), shape((rows_o * nf, half), bf16), shape((2 * half, tokens))],
    )(place, inputs, attended, proj_query, proj_output, own, *[near[m] for m in range(1, nr)])
    oth_q, oth_o = over_tp(all_q), over_tp(all_o)

    mine = {m: over_rep(red, m) for m in rep_order}
    mine[0] = red
    other = {m: over_tp(mine[m]) for m in range(nr)}
    parts = call(
        lambda *a: low_kernel(nf, nr, block_q, *a),
        "low",
        [shape((rows, block))] * nf,
        scratch=[pltpu.VMEM((rank, block), f32)],
    )(place, *[cots[m] for m in range(nr)], *[mine[m] for m in range(nr)], *[other[m] for m in range(nr)])
    got = {m: over_fs(parts[m], m) for m in fs_order}
    moments = (first_query, second_query, first_output, second_output)
    low, half_block = call(
        lambda *a: moment_kernel(nf, block_q, *a),
        "moment",
        [shape((rows, block)), shape((rows + TAIL, block), bf16)],
    )(place, parts[0], *[got[m] for m in range(1, nf)], *moments)

    half_far = {m: over_fs(half_block, m) for m in fs_order}
    half_own = jnp.concatenate([half_block] + [half_far[m] for m in range(1, nf)], axis=0)
    halves = {m: over_rep(half_own, m) for m in rep_order}
    halves[0] = half_own

    lows = {m: over_rep(low, m) for m in rep_order}
    lows[0] = low
    new_state = call(
        lambda *a: state_kernel(nr, block_q, *a),
        "state",
        [shape((rows, cols_q))] * 2 + [shape((rows, cols_o))] * 2,
    )(place, *[lows[m] for m in range(nr)], *moments)

    total = jnp.zeros((), f32)
    for m in range(nr):
        for z in range(nf):
            base = z * (rows + TAIL) + rows
            total = total + jnp.sum(halves[m][base : base + 3, 0].astype(f32))
    total = total + over_tp(jnp.full((8, 128), total))[0, 0]
    scale = lax.rsqrt(total / (rank * (cols_q + cols_o) * 2) + mean_eps).reshape(1)

    decoded = jnp.stack([codes[m] for m in range(nr)]).astype(f32) * (1.0 / code_scale)

    def whole(x):
        return pl.BlockSpec(x.shape, lambda mr, mz, place, scale: (0,) * x.ndim)

    half_list = [halves[m] for m in range(nr)]
    here_q = pl.BlockSpec((part_q, cols_q), lambda mr, mz, place, scale: (place[1] ^ mr, 0))
    here_o = pl.BlockSpec((part_o, cols_o), lambda mr, mz, place, scale: (place[1] ^ mr, 0))
    there_q = pl.BlockSpec((part_q, cols_q), lambda mr, mz, place, scale: ((place[0] ^ mz) * nr + (place[1] ^ mr), 0))
    there_o = pl.BlockSpec((part_o, cols_o), lambda mr, mz, place, scale: ((place[0] ^ mz) * nr + (place[1] ^ mr), 0))
    copy_q, copy_o, new_q, new_o, step_q, step_o = pl.pallas_call(
        lambda *a: step_kernel(nf, nr, block_q, *a),
        grid_spec=pltpu.PrefetchScalarGridSpec(
            num_scalar_prefetch=2,
            grid=(nr, nf),
            in_specs=[whole(x) for x in (all_q, all_o, oth_q, oth_o, *half_list)]
            + [
                pl.BlockSpec((1, 1, *code.shape), lambda mr, mz, place, scale: (mr, jnp.maximum(mz, 1) - 1, 0, 0)),
                here_q,
                here_o,
            ],
            out_specs=[there_q, there_o, here_q, here_o, here_q, here_o],
            scratch_shapes=[pltpu.VMEM((rank, cols_q), bf16), pltpu.VMEM((rank, cols_o), bf16)],
        ),
        out_shape=[
            shape((rows_q * nf, cols_q), bf16),
            shape((rows_o * nf, cols_o), bf16),
            shape((rows_q, cols_q)),
            shape((rows_o, cols_o)),
            shape((rows_q, cols_q)),
            shape((rows_o, cols_o)),
        ],
        name="step",
    )(place, scale, all_q, all_o, oth_q, oth_o, *half_list, decoded, weight_query, weight_output)
    return (new_q, new_o, step_q, step_o, *(new_state[k] for k in (0, 1, 2, 3)), copy_q, copy_o)


def solution(mesh):
    nf, nr, nt = (mesh.shape[a] for a in ("fs", "rep", "tp"))

    def local(*args):
        rows_o = args[5].shape[0]
        rank = args[4].shape[1]
        short = nt == 2 and nf in (2, 4) and nr in (2, 4) and rows_o % (16 * nr) == 0 and rank % (256) == 0
        if short:
            return local_short(nf, nr, *args)
        return local_general(*args)

    spec = P("fs", "tp")
    return jax.shard_map(
        local,
        mesh=mesh,
        in_specs=(
            P(("fs", "rep"), None),
            P(("fs", "rep"), "tp"),
            P(("fs", "rep"), None),
            P(("fs", "rep"), "tp"),
            P("fs", None),
            P("fs", None),
        )
        + (spec,) * 6,
        out_specs=(spec,) * 8 + (P(None, "tp"), P(None, "tp")),
        check_vma=False,
    )
```

```python
import jax
import jax.numpy as jnp
from jax import lax
from jax.experimental import pallas as pl
from jax.experimental.pallas import tpu as pltpu
from jax.sharding import PartitionSpec as P

beta_first = 0.9
beta_second = 0.95
adam_eps = 1e-08
mean_eps = 1e-06
learn_rate = 0.02
code_scale = 2.0**17


f32 = jnp.float32
bf16 = jnp.bfloat16
VMEM = pl.BlockSpec(memory_space=pltpu.VMEM)
SMEM = pl.BlockSpec(memory_space=pltpu.SMEM)
ANY = pl.BlockSpec(memory_space=pl.ANY)
HBM = pl.BlockSpec(memory_space=pltpu.HBM)
TAIL = 16
MIB = 2**20


def moment_update(low_sum, first, second):
    first_new = beta_first * first + (1.0 - beta_first) * low_sum
    second_new = beta_second * second + (1.0 - beta_second) * low_sum * low_sum
    normed = first_new / (jnp.sqrt(second_new) + adam_eps)
    return (first_new, second_new, normed)


def contract_rows(left, right):
    return lax.dot_general(
        left,
        right,
        (((0,), (0,)), ((), ())),
        precision=lax.Precision.HIGHEST,
        preferred_element_type=f32,
    )


def local_general(inputs, query_cot, attended, output_cot, proj_query, proj_output, weight_query, weight_output, first_query, second_query, first_output, second_output):
    def gather(x):
        return lax.all_gather(x, "fs", axis=0, tiled=True)

    def low_of(acts, proj, cot):
        reduced = jnp.dot(acts, gather(proj), preferred_element_type=f32)
        part = contract_rows(reduced, cot.astype(f32))
        return lax.psum_scatter(part, "fs", scatter_dimension=0, tiled=True)

    low_query, low_output = lax.psum((low_of(inputs, proj_query, query_cot), low_of(attended, proj_output, output_cot)), "rep")
    first_q, second_q, normed_q = moment_update(low_query, first_query, second_query)
    first_o, second_o, normed_o = moment_update(low_output, first_output, second_output)
    total = lax.psum(jnp.sum(normed_q * normed_q) + jnp.sum(normed_o * normed_o), ("fs", "tp"))
    entries = (normed_q.size + normed_o.size) * lax.axis_size("fs") * lax.axis_size("tp")
    scale = lax.rsqrt(total / entries + mean_eps)
    step_q = scale * jnp.dot(proj_query, gather(normed_q.astype(bf16)), preferred_element_type=f32)
    step_o = scale * jnp.dot(proj_output, gather(normed_o.astype(bf16)), preferred_element_type=f32)
    new_q = weight_query - learn_rate * step_q
    new_o = weight_output - learn_rate * step_o
    return (new_q, new_o, step_q, step_o, first_q, second_q, first_o, second_o, gather(new_q.astype(bf16)), gather(new_o.astype(bf16)))


def fetch(pairs, sems):
    copies = [pltpu.make_async_copy(src, dst, sems.at[k]) for k, (src, dst) in enumerate(pairs)]
    for copy in copies:
        copy.start()
    for copy in copies:
        copy.wait()


def share_kernel(nr, place, proj_q, proj_o, out, sems):
    r, t = place[1], place[2]
    part_q, part_o, half = proj_q.shape[0] // nr, proj_o.shape[0] // nr, out.shape[1]
    mine = pl.ds(pl.multiple_of(t * half, half), half)
    fetch(
        [
            (proj_q.at[pl.ds(pl.multiple_of(r * part_q, part_q), part_q), mine], out.at[0:part_q, :]),
            (proj_o.at[pl.ds(pl.multiple_of(r * part_o, part_o), part_o), mine], out.at[part_q : part_q + part_o, :]),
        ],
        sems,
    )


def cot_kernel(nr, place, cot_q, cot_o, *rest):
    outs, sems = rest[:-1], rest[-1]
    r = place[1]
    block_q, block_o = cot_q.shape[1] // nr, cot_o.shape[1] // nr
    pairs = []
    for m, out in enumerate(outs):
        at = r ^ m
        pairs.append((cot_q.at[:, pl.ds(pl.multiple_of(at * block_q, block_q), block_q)], out.at[:, 0:block_q]))
        pairs.append((cot_o.at[:, pl.ds(pl.multiple_of(at * block_o, block_o), block_o)], out.at[:, block_q : block_q + block_o]))
    fetch(pairs, sems)


def cut_kernel(nr, place, weight_q, weight_o, out, sems):
    at = place[1] ^ (nr - 1)
    part_q, part_o = weight_q.shape[0] // nr, weight_o.shape[0] // nr
    cols = weight_q.shape[1]
    pairs = [(weight_q.at[pl.ds(pl.multiple_of(at * part_q, part_q), part_q), :], out.at[0:part_q, :])]
    for k in range(weight_o.shape[1] // cols):
        base = part_q + k * part_o
        rows = pl.ds(pl.multiple_of(at * part_o, part_o), part_o)
        pairs.append((weight_o.at[rows, k * cols : (k + 1) * cols], out.at[base : base + part_o, :]))
    fetch(pairs, sems)


def reduce_kernel(nf, nr, place, inputs, attended, proj_q, proj_o, own, *rest):
    near, (table, red) = rest[:-2], rest[-2:]
    f, r, t = place[0], place[1], place[2]
    half = table.shape[1]
    rows_q, rows_o = proj_q.shape[0], proj_o.shape[0]
    part_q, part_o = rows_q // nr, rows_o // nr
    part = part_q + part_o
    cut = nf * rows_q
    mine = pl.ds(pl.multiple_of(t * half, half), half)
    table[pl.ds(pl.multiple_of(f * rows_q, rows_q), rows_q), :] = proj_q[:, mine]
    table[pl.ds(pl.multiple_of(cut + f * rows_o, rows_o), rows_o), :] = proj_o[:, mine]
    for mr, ref in enumerate((own,) + near):
        for mz in range(1, nf):
            at = (f ^ mz) * nr + (r ^ mr)
            base = (mz - 1) * part
            table[pl.ds(pl.multiple_of(at * part_q, part_q), part_q), :] = ref[base : base + part_q, :]
            table[pl.ds(pl.multiple_of(cut + at * part_o, part_o), part_o), :] = ref[base + part_q : base + part, :]
    red_q = jnp.dot(inputs[...], table[0:cut, :], preferred_element_type=f32)
    red_o = jnp.dot(attended[...], table[cut:, :], preferred_element_type=f32)
    red[0:half, :] = red_q.T
    red[half : 2 * half, :] = red_o.T


def split_three(x):
    high = x.astype(bf16)
    rest = x - high.astype(f32)
    mid = rest.astype(bf16)
    return high, mid, (rest - mid.astype(f32)).astype(bf16)


def low_kernel(nf, nr, block_q, place, *refs):
    cots, mine, other, outs, low = refs[:nr], refs[nr : 2 * nr], refs[2 * nr : 3 * nr], refs[3 * nr : 3 * nr + nf], refs[-1]
    f, t = place[0], place[2]
    half = mine[0].shape[0] // 2
    cot = jnp.concatenate([c[...] for c in cots], axis=0)
    for which, group in enumerate((mine, other)):
        top = pl.multiple_of((t ^ which) * half, half)
        for k, (lo, hi) in enumerate(((0, block_q), (block_q, cot.shape[1]))):
            left = jnp.concatenate([g[k * half : (k + 1) * half, :] for g in group], axis=1)
            acc = None
            for term in split_three(left):
                got = jnp.dot(term, cot[:, lo:hi], preferred_element_type=f32)
                acc = got if acc is None else acc + got
            low[pl.ds(top, half), lo:hi] = acc
    rows = low.shape[0] // nf
    for m in range(nf):
        outs[m][...] = low[pl.ds(pl.multiple_of((f ^ m) * rows, rows), rows), :]


def pack_total(spread):
    row = lax.broadcasted_iota(jnp.int32, spread.shape, 0)
    high, mid, last = (x.astype(f32) for x in split_three(spread))
    packed = jnp.where(row == 0, high, jnp.where(row == 1, mid, jnp.where(row == 2, last, 0.0)))
    return jnp.concatenate([packed, jnp.zeros_like(packed)], axis=0).astype(bf16)


def add_totals(tails):
    acc = tails[0].astype(f32)
    for tail in tails[1:]:
        acc = acc + tail.astype(f32)
    return jnp.sum(acc, axis=0, keepdims=True)


def moment_kernel(nf, block_q, place, *refs):
    parts, (first_q, second_q, first_o, second_o, low_out, half_out) = refs[:nf], refs[nf:]
    r = place[1]
    low = parts[0][...]
    for p in parts[1:]:
        low = low + p[...]
    low_out[...] = low
    block_o = low.shape[1] - block_q
    rows = low.shape[0]
    total = jnp.zeros((), f32)
    for first, second, lo, width in ((first_q, second_q, 0, block_q), (first_o, second_o, block_q, block_o)):
        cols = pl.ds(pl.multiple_of(r * width, width), width)
        _, _, normed = moment_update(low[:, lo : lo + width], first[:, cols], second[:, cols])
        half_out[0:rows, lo : lo + width] = normed.astype(bf16)
        total = total + jnp.sum(normed * normed)
    half_out[rows : rows + TAIL, :] = pack_total(jnp.full((8, low.shape[1]), total, f32))


def line_kernel(nf, place, *refs):
    blocks, (table, total) = refs[:nf], refs[nf:]
    f = place[0]
    rows = blocks[0].shape[0] - TAIL
    for m, block in enumerate(blocks):
        table[pl.ds(pl.multiple_of((f ^ m) * rows, rows), rows), :] = block[0:rows, :]
    found = add_totals([block[rows : rows + TAIL, 0 : total.shape[1]] for block in blocks])
    total[...] = jnp.broadcast_to(found, total.shape)


def left_kernel(place, mine, other, out):
    t = place[2]
    half = mine.shape[1]
    out[:, pl.ds(pl.multiple_of(t * half, half), half)] = mine[...]
    out[:, pl.ds(pl.multiple_of((1 - t) * half, half), half)] = other[...]


def step_kernel(nf, nr, block_q, count, place, left, *rest):
    halves, totals, lows, rest = rest[:nr], rest[nr : 2 * nr], rest[2 * nr : 3 * nr], rest[3 * nr :]
    codes, near, rest = rest[: nr - 1], rest[nr - 1], rest[nr:]
    first_q, second_q, first_o, second_o, weight_q, weight_o = rest[:6]
    copy_q, copy_o, new_q, new_o, step_q, step_o, new_fq, new_sq, new_fo, new_so, table, scale_out = rest[6:18]
    made_q, made_o, fresh_q, fresh_o, moved_q, moved_o, got_q, got_o, made_fq, made_sq, made_fo, made_so, sems = rest[18:]
    f, r = place[0], place[1]
    rows_q, cols_q = weight_q.shape
    rows_o, cols_o = weight_o.shape
    part_q, part_o = rows_q // nr, rows_o // nr
    cut = nf * rows_q
    block_o = cols_o // nr
    total = totals[0][...]
    for x in totals[1:]:
        total = total + x[...]
    scale = lax.rsqrt(total / count + mean_eps)
    scale_out[...] = scale
    scale = scale[0:1, 0:1]

    for m in range(nr):
        at = r ^ m
        table[:, pl.ds(pl.multiple_of(at * block_q, block_q), block_q)] = halves[m][:, 0:block_q]
        table[:, pl.ds(pl.multiple_of(cols_q + at * block_o, block_o), block_o)] = halves[m][:, block_q:]

    pending = []

    def send(src, dst):
        copy = pltpu.make_async_copy(src, dst, sems.at[len(pending)])
        copy.start()
        pending.append(copy)

    for mz in range(nf):
        at_q = pl.ds(pl.multiple_of((f ^ mz) * rows_q, rows_q), rows_q)
        at_o = pl.ds(pl.multiple_of((f ^ mz) * rows_o, rows_o), rows_o)
        left_o = pl.ds(pl.multiple_of(cut + (f ^ mz) * rows_o, rows_o), rows_o)
        found_q = scale * jnp.dot(left[at_q, :], table[:, 0:cols_q], preferred_element_type=f32)
        if mz == 0:
            moved_q[...] = found_q
            fresh_q[...] = weight_q[...] - learn_rate * found_q
            made_q[at_q, :] = fresh_q[...].astype(bf16)
            send(moved_q, step_q)
            send(fresh_q, new_q)
            send(made_q.at[at_q, :], copy_q.at[at_q, :])
        else:
            got_q[...] = found_q
            for mr in range(nr if mz == 1 else nr - 1):
                at = (r ^ mr) * part_q
                old = codes[mr][mz - 1, 0:part_q, :] if mr < nr - 1 else near[0:part_q, :]
                to = pl.ds(pl.multiple_of((f ^ mz) * rows_q + at, part_q), part_q)
                made_q[to, :] = (old - learn_rate * got_q[pl.ds(pl.multiple_of(at, part_q), part_q), :]).astype(bf16)
                send(made_q.at[to, :], copy_q.at[to, :])
        found_o = scale * jnp.dot(left[left_o, :], table[:, cols_q:], preferred_element_type=f32)
        if mz == 0:
            moved_o[...] = found_o
            fresh_o[...] = weight_o[...] - learn_rate * found_o
            made_o[at_o, :] = fresh_o[...].astype(bf16)
            send(moved_o, step_o)
            send(fresh_o, new_o)
            send(made_o.at[at_o, :], copy_o.at[at_o, :])
        else:
            got_o[...] = found_o
            for mr in range(nr if mz == 1 else nr - 1):
                at = (r ^ mr) * part_o
                to = pl.ds(pl.multiple_of((f ^ mz) * rows_o + at, part_o), part_o)
                for k in range(cols_o // cols_q):
                    base = part_q + k * part_o
                    lo = k * cols_q
                    old = codes[mr][mz - 1, base : base + part_o, :] if mr < nr - 1 else near[base : base + part_o, :]
                    made_o[to, lo : lo + cols_q] = (
                        old - learn_rate * got_o[pl.ds(pl.multiple_of(at, part_o), part_o), lo : lo + cols_q]
                    ).astype(bf16)
                send(made_o.at[to, :], copy_o.at[to, :])
    for first, second, made_f, made_s, new_f, new_s, lo, width in (
        (first_q, second_q, made_fq, made_sq, new_fq, new_sq, 0, block_q),
        (first_o, second_o, made_fo, made_so, new_fo, new_so, block_q, block_o),
    ):
        for m in range(nr):
            cols = pl.ds(pl.multiple_of((r ^ m) * width, width), width)
            first_new, second_new, _ = moment_update(lows[m][:, lo : lo + width], first[:, cols], second[:, cols])
            made_f[:, cols] = first_new
            made_s[:, cols] = second_new
        send(made_f, new_f)
        send(made_s, new_s)
    for copy in pending:
        copy.wait()


def corner_kernel(nf, nr, place, left, table, scale, tops, ends, had_q, had_o, copy_q, copy_o, made_q, made_o, sems):
    f, r = place[0], place[1]
    scale = scale[0:1, 0:1]
    cols_q = copy_q.shape[1]
    cols_o = copy_o.shape[1]
    part_q = made_q.shape[0] // (nf - 2)
    part_o = made_o.shape[0] // (nf - 2)
    cut = nf * nr * part_q
    pending = []
    for k, mz in enumerate(range(2, nf)):
        at = (f ^ mz) * nr + (r ^ (nr - 1))
        to_q = pl.ds(pl.multiple_of(at * part_q, part_q), part_q)
        to_o = pl.ds(pl.multiple_of(at * part_o, part_o), part_o)
        got = scale * jnp.dot(left[to_q, :], table[:, 0:cols_q], preferred_element_type=f32)
        here_q = pl.ds(k * part_q, part_q)
        made_q[here_q, :] = (tops[here_q, :] - learn_rate * got).astype(bf16)
        copy = pltpu.make_async_copy(made_q.at[here_q, :], copy_q.at[to_q, :], sems.at[2 * k])
        copy.start()
        pending.append(copy)
        from_o = pl.ds(pl.multiple_of(cut + at * part_o, part_o), part_o)
        got = scale * jnp.dot(left[from_o, :], table[:, cols_q:], preferred_element_type=f32)
        here_o = pl.ds(k * part_o, part_o)
        for c in range(cols_o // cols_q):
            old = ends[pl.ds(k * part_q + c * part_o, part_o), :]
            lo = c * cols_q
            made_o[here_o, lo : lo + cols_q] = (old - learn_rate * got[:, lo : lo + cols_q]).astype(bf16)
        copy = pltpu.make_async_copy(made_o.at[here_o, :], copy_o.at[to_o, :], sems.at[2 * k + 1])
        copy.start()
        pending.append(copy)
    for copy in pending:
        copy.wait()


def shape(x, dtype=f32):
    return jax.ShapeDtypeStruct(tuple(x), dtype)


def call(kernel, outs, args, scratch=(), limit=6 * MIB, places=VMEM, source=VMEM):
    many = isinstance(outs, list)
    return pl.pallas_call(
        kernel,
        out_shape=outs,
        in_specs=[SMEM] + [source] * (len(args) - 1),
        out_specs=[places] * len(outs) if many else places,
        scratch_shapes=scratch,
        compiler_params=pltpu.CompilerParams(vmem_limit_bytes=limit),
    )(*args)


def local_short(nf, nr, inputs, query_cot, attended, output_cot, proj_query, proj_output, weight_query, weight_output, first_query, second_query, first_output, second_output):
    f, r, t = (lax.axis_index(a) for a in ("fs", "rep", "tp"))
    place = jnp.stack([f, r, t]).astype(jnp.int32)
    hold = lax.optimization_barrier

    def swap(x, axis, m, n):
        return lax.ppermute(x, axis, [(i, i ^ m) for i in range(n)])

    fs_order = list(range(nf - 1, 0, -1))
    rep_order = list(range(nr - 1, 0, -1))

    def over_fs(make):
        got = {m: swap(make(m), "fs", m, nf) for m in fs_order}
        return [got[m] for m in range(1, nf)]

    def over_rep(make):
        got = {m: swap(make(m), "rep", m, nr) for m in rep_order}
        return [got[m] for m in range(1, nr)]

    def over_tp(x):
        return swap(x, "tp", 1, 2)

    tokens = inputs.shape[0]
    rank = proj_query.shape[1]
    half = rank // 2
    rows_q, rows_o = proj_query.shape[0], proj_output.shape[0]
    part_q, part_o = rows_q // nr, rows_o // nr
    cols_q, cols_o = query_cot.shape[1], output_cot.shape[1]
    block_q, block_o = cols_q // nr, cols_o // nr
    block = block_q + block_o
    rows = rank // nf

    share = call(
        lambda *a: share_kernel(nr, *a),
        shape((part_q + part_o, half), bf16),
        (place, proj_query, proj_output),
        scratch=[pltpu.SemaphoreType.DMA((2,))],
        source=ANY,
    )
    far = over_fs(lambda m: share)

    def encode(at, old_q, old_o):
        parts = [lax.dynamic_slice(old_q, (at * part_q, 0), (part_q, cols_q))]
        for k in range(cols_o // cols_q):
            parts.append(lax.dynamic_slice(old_o, (at * part_o, k * cols_q), (part_o, cols_q)))
        return (jnp.concatenate(parts, axis=0) * code_scale).astype(jnp.float16)

    code = encode(r, weight_query, weight_output)
    code_far = {m: swap(code, "fs", m, nf) for m in range(1, nf)}

    cots = call(
        lambda *a: cot_kernel(nr, *a),
        [shape((tokens, block), bf16)] * nr,
        (place, query_cot, output_cot),
        scratch=[pltpu.SemaphoreType.DMA((2 * nr,))],
        source=ANY,
    )
    cots = [cots[0]] + over_rep(lambda m: cots[m])

    corner = call(
        lambda *a: cut_kernel(nr, *a),
        shape(code.shape),
        (place, weight_query, weight_output),
        scratch=[pltpu.SemaphoreType.DMA((1 + cols_o // cols_q,))],
        source=ANY,
    )
    corner = (corner * code_scale).astype(jnp.float16)
    corners = {1: swap(corner, "fs", 1, nf)}

    own = jnp.concatenate(far, axis=0)
    near = over_rep(lambda m: own)

    table, red = call(
        lambda *a: reduce_kernel(nf, nr, *a),
        [shape(((rows_q + rows_o) * nf, half), bf16), shape((2 * half, tokens))],
        (place, inputs, attended, proj_query, proj_output, own, *near),
    )
    mine = [red] + over_rep(lambda m: red)
    other = [over_tp(x) for x in mine]
    parts = call(
        lambda *a: low_kernel(nf, nr, block_q, *a),
        [shape((rows, block))] * nf,
        (place, *cots, *mine, *other),
        scratch=[pltpu.VMEM((rank, block), f32)],
    )
    got = over_fs(lambda m: parts[m])

    def spread(piece):
        return swap(piece, "rep", 1, nr), swap(piece, "rep", 2, nr)

    later = hold((parts[0], *(code_far[m] for m in range(2, nf))))[1:]
    pieces = {1: code_far[1], **dict(zip(range(2, nf), later))}
    pairs = {m: spread(pieces[m]) for m in range(1, nf)}
    tops = swap(jnp.concatenate([pairs[m][0][:part_q] for m in range(2, nf)], axis=0), "rep", 2, nr)
    ends = swap(jnp.concatenate([pairs[m][1][part_q:] for m in range(2, nf)], axis=0), "rep", 1, nr)

    moments = (first_query, second_query, first_output, second_output)
    low, half_block = call(
        lambda *a: moment_kernel(nf, block_q, *a),
        [shape((rows, block)), shape((rows + TAIL, block), bf16)],
        (place, parts[0], *got, *moments),
    )
    half_far = over_fs(lambda m: half_block)
    other_table = over_tp(table)
    left = call(left_kernel, shape(((rows_q + rows_o) * nf, rank), bf16), (place, table, other_table))
    half_own, line = call(
        lambda *a: line_kernel(nf, *a), [shape((rank, block), bf16), shape((8, 128))], (place, half_block, *half_far)
    )
    halves = [half_own] + over_rep(lambda m: half_own)
    line = line + over_tp(line)
    totals = [line] + over_rep(lambda m: line)
    lows = [low] + over_rep(lambda m: low)
    near = hold((pieces[1], *pairs[1], corners[1], half_own))[:-1]
    pieces[1], pairs[1], corners[1] = near[0], near[1:3], near[3]

    def decode(x):
        return x.astype(f32) * (1.0 / code_scale)

    groups = ([pieces[m], *pairs[m]] for m in range(1, nf))
    codes = [decode(jnp.stack(x)) for x in zip(*groups)]
    count = rank * (cols_q + cols_o) * 2
    copy_q, copy_o, new_q, new_o, step_q, step_o, *new_state, all_half, scale = pl.pallas_call(
        lambda *a: step_kernel(nf, nr, block_q, count, *a),
        out_shape=[
            shape((rows_q * nf, cols_q), bf16),
            shape((rows_o * nf, cols_o), bf16),
            shape((rows_q, cols_q)),
            shape((rows_o, cols_o)),
            shape((rows_q, cols_q)),
            shape((rows_o, cols_o)),
            *[shape((rows, cols_q))] * 2,
            *[shape((rows, cols_o))] * 2,
            shape((rank, cols_q + cols_o), bf16),
            shape((8, 128)),
        ],
        in_specs=[SMEM] + [VMEM] * (4 * nr + 7),
        out_specs=[ANY] * 10 + [VMEM] * 2,
        scratch_shapes=[
            pltpu.VMEM((rows_q * nf, cols_q), bf16),
            pltpu.VMEM((rows_o * nf, cols_o), bf16),
            pltpu.VMEM((rows_q, cols_q), f32),
            pltpu.VMEM((rows_o, cols_o), f32),
            pltpu.VMEM((rows_q, cols_q), f32),
            pltpu.VMEM((rows_o, cols_o), f32),
            pltpu.VMEM((rows_q, cols_q), f32),
            pltpu.VMEM((rows_o, cols_o), f32),
            *[pltpu.VMEM((rows, cols_q), f32)] * 2,
            *[pltpu.VMEM((rows, cols_o), f32)] * 2,
            pltpu.SemaphoreType.DMA((10 + 2 * nr * (nf - 1),)),
        ],
        name="step",
        compiler_params=pltpu.CompilerParams(vmem_limit_bytes=24 * MIB),
    )(place, left, *halves, *totals, *lows, *codes, decode(corners[1]), *moments, weight_query, weight_output)
    tops, ends = hold((tops, ends, scale))[:2]
    copy_q, copy_o = pl.pallas_call(
        lambda *a: corner_kernel(nf, nr, *a),
        out_shape=[shape(copy_q.shape, bf16), shape(copy_o.shape, bf16)],
        in_specs=[SMEM] + [VMEM] * 5 + [ANY] * 2,
        out_specs=[ANY] * 2,
        scratch_shapes=[
            pltpu.VMEM(((nf - 2) * part_q, cols_q), bf16),
            pltpu.VMEM(((nf - 2) * part_o, cols_o), bf16),
            pltpu.SemaphoreType.DMA((2 * (nf - 2),)),
        ],
        input_output_aliases={6: 0, 7: 1},
        name="corner",
        compiler_params=pltpu.CompilerParams(vmem_limit_bytes=6 * MIB),
    )(place, left, all_half, scale, decode(tops), decode(ends), copy_q, copy_o)
    return (new_q, new_o, step_q, step_o, *new_state, copy_q, copy_o)


def solution(mesh):
    nf, nr, nt = (mesh.shape[a] for a in ("fs", "rep", "tp"))

    def local(*args):
        rows_o = args[5].shape[0]
        rank = args[4].shape[1]
        if nt == 2 and nf == 4 and nr == 4 and rows_o % (16 * nr) == 0 and rank % 256 == 0:
            return local_short(nf, nr, *args)
        return local_general(*args)

    spec = P("fs", "tp")
    return jax.shard_map(
        local,
        mesh=mesh,
        in_specs=(
            P(("fs", "rep"), None),
            P(("fs", "rep"), "tp"),
            P(("fs", "rep"), None),
            P(("fs", "rep"), "tp"),
            P("fs", None),
            P("fs", None),
        )
        + (spec,) * 6,
        out_specs=(spec,) * 8 + (P(None, "tp"), P(None, "tp")),
        check_vma=False,
    )
```

```python
import jax
import jax.numpy as jnp
from jax import lax
from jax.experimental import pallas as pl
from jax.experimental.pallas import tpu as pltpu
from jax.sharding import PartitionSpec as P

beta_first = 0.9
beta_second = 0.95
adam_eps = 1e-08
mean_eps = 1e-06
learn_rate = 0.02
code_scale = 2.0**17


f32 = jnp.float32
bf16 = jnp.bfloat16
VMEM = pl.BlockSpec(memory_space=pltpu.VMEM)
SMEM = pl.BlockSpec(memory_space=pltpu.SMEM)
ANY = pl.BlockSpec(memory_space=pl.ANY)
HBM = pl.BlockSpec(memory_space=pltpu.HBM)
TAIL = 16
MIB = 2**20


def moment_update(low_sum, first, second):
    first_new = beta_first * first + (1.0 - beta_first) * low_sum
    second_new = beta_second * second + (1.0 - beta_second) * low_sum * low_sum
    normed = first_new / (jnp.sqrt(second_new) + adam_eps)
    return (first_new, second_new, normed)


def contract_rows(left, right):
    return lax.dot_general(
        left,
        right,
        (((0,), (0,)), ((), ())),
        precision=lax.Precision.HIGHEST,
        preferred_element_type=f32,
    )


def local_general(inputs, query_cot, attended, output_cot, proj_query, proj_output, weight_query, weight_output, first_query, second_query, first_output, second_output):
    def gather(x):
        return lax.all_gather(x, "fs", axis=0, tiled=True)

    def low_of(acts, proj, cot):
        reduced = jnp.dot(acts, gather(proj), preferred_element_type=f32)
        part = contract_rows(reduced, cot.astype(f32))
        return lax.psum_scatter(part, "fs", scatter_dimension=0, tiled=True)

    low_query, low_output = lax.psum((low_of(inputs, proj_query, query_cot), low_of(attended, proj_output, output_cot)), "rep")
    first_q, second_q, normed_q = moment_update(low_query, first_query, second_query)
    first_o, second_o, normed_o = moment_update(low_output, first_output, second_output)
    total = lax.psum(jnp.sum(normed_q * normed_q) + jnp.sum(normed_o * normed_o), ("fs", "tp"))
    entries = (normed_q.size + normed_o.size) * lax.axis_size("fs") * lax.axis_size("tp")
    scale = lax.rsqrt(total / entries + mean_eps)
    step_q = scale * jnp.dot(proj_query, gather(normed_q.astype(bf16)), preferred_element_type=f32)
    step_o = scale * jnp.dot(proj_output, gather(normed_o.astype(bf16)), preferred_element_type=f32)
    new_q = weight_query - learn_rate * step_q
    new_o = weight_output - learn_rate * step_o
    return (new_q, new_o, step_q, step_o, first_q, second_q, first_o, second_o, gather(new_q.astype(bf16)), gather(new_o.astype(bf16)))


def fetch(pairs, sems):
    copies = [pltpu.make_async_copy(src, dst, sems.at[k]) for k, (src, dst) in enumerate(pairs)]
    for copy in copies:
        copy.start()
    for copy in copies:
        copy.wait()


def share_kernel(nr, place, proj_q, proj_o, share, both, sems):
    r, t = place[1], place[2]
    part_q, part_o, half = proj_q.shape[0] // nr, proj_o.shape[0] // nr, share.shape[1]
    part = part_q + part_o
    mine = pl.ds(pl.multiple_of(t * half, half), half)
    pairs = []
    for at, out, base in ((r, share, 0), (r, both, 0), (r ^ (nr - 1), both, part)):
        pairs.append((proj_q.at[pl.ds(pl.multiple_of(at * part_q, part_q), part_q), mine], out.at[base : base + part_q, :]))
        pairs.append((proj_o.at[pl.ds(pl.multiple_of(at * part_o, part_o), part_o), mine], out.at[base + part_q : base + part, :]))
    fetch(pairs, sems)


def cot_kernel(nr, place, cot_q, cot_o, *rest):
    outs, sems = rest[:-1], rest[-1]
    r = place[1]
    block_q, block_o = cot_q.shape[1] // nr, cot_o.shape[1] // nr
    pairs = []
    for m, out in enumerate(outs):
        at = r ^ m
        pairs.append((cot_q.at[:, pl.ds(pl.multiple_of(at * block_q, block_q), block_q)], out.at[:, 0:block_q]))
        pairs.append((cot_o.at[:, pl.ds(pl.multiple_of(at * block_o, block_o), block_o)], out.at[:, block_q : block_q + block_o]))
    fetch(pairs, sems)


def cut_kernel(nr, place, weight_q, weight_o, out, sems):
    at = place[1] ^ (nr - 1)
    part_q, part_o = weight_q.shape[0] // nr, weight_o.shape[0] // nr
    cols = weight_q.shape[1]
    pairs = [(weight_q.at[pl.ds(pl.multiple_of(at * part_q, part_q), part_q), :], out.at[0:part_q, :])]
    for k in range(weight_o.shape[1] // cols):
        base = part_q + k * part_o
        rows = pl.ds(pl.multiple_of(at * part_o, part_o), part_o)
        pairs.append((weight_o.at[rows, k * cols : (k + 1) * cols], out.at[base : base + part_o, :]))
    fetch(pairs, sems)


def reduce_kernel(nf, nr, place, inputs, attended, proj_q, proj_o, own, *rest):
    near, (both, table, red) = rest[:-3], rest[-3:]
    f, r, t = place[0], place[1], place[2]
    half = table.shape[1]
    rows_q, rows_o = proj_q.shape[0], proj_o.shape[0]
    part_q, part_o = rows_q // nr, rows_o // nr
    part = part_q + part_o
    cut = nf * rows_q
    mine = pl.ds(pl.multiple_of(t * half, half), half)
    table[pl.ds(pl.multiple_of(f * rows_q, rows_q), rows_q), :] = proj_q[:, mine]
    table[pl.ds(pl.multiple_of(cut + f * rows_o, rows_o), rows_o), :] = proj_o[:, mine]
    for mr, whole in enumerate((own,) + near):
        for mz in range(1, nf):
            at = (f ^ mz) * nr + (r ^ mr)
            ref, base = whole, (mz - 1) * part
            if mr == nr - 1:
                ref, base = (both, part) if mz == 1 else (whole, base - part)
            table[pl.ds(pl.multiple_of(at * part_q, part_q), part_q), :] = ref[base : base + part_q, :]
            table[pl.ds(pl.multiple_of(cut + at * part_o, part_o), part_o), :] = ref[base + part_q : base + part, :]
    red_q = jnp.dot(inputs[...], table[0:cut, :], preferred_element_type=f32)
    red_o = jnp.dot(attended[...], table[cut:, :], preferred_element_type=f32)
    red[0:half, :] = red_q.T
    red[half : 2 * half, :] = red_o.T


def split_three(x):
    high = x.astype(bf16)
    rest = x - high.astype(f32)
    mid = rest.astype(bf16)
    return high, mid, (rest - mid.astype(f32)).astype(bf16)


def low_kernel(nf, nr, block_q, place, *refs):
    cots, mine, other, outs, low = refs[:nr], refs[nr : 2 * nr], refs[2 * nr : 3 * nr], refs[3 * nr : 3 * nr + nf], refs[-1]
    f, t = place[0], place[2]
    half = mine[0].shape[0] // 2
    cot = jnp.concatenate([c[...] for c in cots], axis=0)
    for which, group in enumerate((mine, other)):
        top = pl.multiple_of((t ^ which) * half, half)
        for k, (lo, hi) in enumerate(((0, block_q), (block_q, cot.shape[1]))):
            left = jnp.concatenate([g[k * half : (k + 1) * half, :] for g in group], axis=1)
            acc = None
            for term in split_three(left):
                got = jnp.dot(term, cot[:, lo:hi], preferred_element_type=f32)
                acc = got if acc is None else acc + got
            low[pl.ds(top, half), lo:hi] = acc
    rows = low.shape[0] // nf
    for m in range(nf):
        outs[m][...] = low[pl.ds(pl.multiple_of((f ^ m) * rows, rows), rows), :]


def pack_total(spread):
    row = lax.broadcasted_iota(jnp.int32, spread.shape, 0)
    high, mid, last = (x.astype(f32) for x in split_three(spread))
    packed = jnp.where(row == 0, high, jnp.where(row == 1, mid, jnp.where(row == 2, last, 0.0)))
    return jnp.concatenate([packed, jnp.zeros_like(packed)], axis=0).astype(bf16)


def add_totals(tails):
    acc = tails[0].astype(f32)
    for tail in tails[1:]:
        acc = acc + tail.astype(f32)
    return jnp.sum(acc, axis=0, keepdims=True)


def moment_kernel(nf, block_q, place, *refs):
    parts, (first_q, second_q, first_o, second_o, low_out, half_out) = refs[:nf], refs[nf:]
    r = place[1]
    low = parts[0][...]
    for p in parts[1:]:
        low = low + p[...]
    low_out[...] = low
    block_o = low.shape[1] - block_q
    rows = low.shape[0]
    total = jnp.zeros((), f32)
    for first, second, lo, width in ((first_q, second_q, 0, block_q), (first_o, second_o, block_q, block_o)):
        cols = pl.ds(pl.multiple_of(r * width, width), width)
        _, _, normed = moment_update(low[:, lo : lo + width], first[:, cols], second[:, cols])
        half_out[0:rows, lo : lo + width] = normed.astype(bf16)
        total = total + jnp.sum(normed * normed)
    half_out[rows : rows + TAIL, :] = pack_total(jnp.full((8, low.shape[1]), total, f32))


def line_kernel(nf, place, *refs):
    blocks, (table, total) = refs[:nf], refs[nf:]
    f = place[0]
    rows = blocks[0].shape[0] - TAIL
    for m, block in enumerate(blocks):
        table[pl.ds(pl.multiple_of((f ^ m) * rows, rows), rows), :] = block[0:rows, :]
    found = add_totals([block[rows : rows + TAIL, 0 : total.shape[1]] for block in blocks])
    total[...] = jnp.broadcast_to(found, total.shape)


def left_kernel(place, mine, other, out):
    t = place[2]
    half = mine.shape[1]
    out[:, pl.ds(pl.multiple_of(t * half, half), half)] = mine[...]
    out[:, pl.ds(pl.multiple_of((1 - t) * half, half), half)] = other[...]


def step_kernel(nf, nr, block_q, count, place, left, *rest):
    halves, totals, lows, rest = rest[:nr], rest[nr : 2 * nr], rest[2 * nr : 3 * nr], rest[3 * nr :]
    codes, near, rest = rest[: nr - 1], rest[nr - 1], rest[nr:]
    first_q, second_q, first_o, second_o, weight_q, weight_o = rest[:6]
    copy_q, copy_o, new_q, new_o, step_q, step_o, new_fq, new_sq, new_fo, new_so, table, scale_out = rest[6:18]
    made_q, made_o, fresh_q, fresh_o, moved_q, moved_o, got_q, got_o, made_fq, made_sq, made_fo, made_so, sems = rest[18:]
    f, r = place[0], place[1]
    rows_q, cols_q = weight_q.shape
    rows_o, cols_o = weight_o.shape
    part_q, part_o = rows_q // nr, rows_o // nr
    cut = nf * rows_q
    block_o = cols_o // nr
    total = totals[0][...]
    for x in totals[1:]:
        total = total + x[...]
    scale = lax.rsqrt(total / count + mean_eps)
    scale_out[...] = scale
    scale = scale[0:1, 0:1]

    for m in range(nr):
        at = r ^ m
        table[:, pl.ds(pl.multiple_of(at * block_q, block_q), block_q)] = halves[m][:, 0:block_q]
        table[:, pl.ds(pl.multiple_of(cols_q + at * block_o, block_o), block_o)] = halves[m][:, block_q:]

    pending = []

    def send(src, dst):
        copy = pltpu.make_async_copy(src, dst, sems.at[len(pending)])
        copy.start()
        pending.append(copy)

    for mz in range(nf):
        at_q = pl.ds(pl.multiple_of((f ^ mz) * rows_q, rows_q), rows_q)
        at_o = pl.ds(pl.multiple_of((f ^ mz) * rows_o, rows_o), rows_o)
        left_o = pl.ds(pl.multiple_of(cut + (f ^ mz) * rows_o, rows_o), rows_o)
        found_q = scale * jnp.dot(left[at_q, :], table[:, 0:cols_q], preferred_element_type=f32)
        if mz == 0:
            moved_q[...] = found_q
            fresh_q[...] = weight_q[...] - learn_rate * found_q
            made_q[at_q, :] = fresh_q[...].astype(bf16)
            send(moved_q, step_q)
            send(fresh_q, new_q)
            send(made_q.at[at_q, :], copy_q.at[at_q, :])
        else:
            got_q[...] = found_q
            for mr in range(nr if mz == 1 else nr - 1):
                at = (r ^ mr) * part_q
                old = codes[mr][mz - 1, 0:part_q, :] if mr < nr - 1 else near[0:part_q, :]
                to = pl.ds(pl.multiple_of((f ^ mz) * rows_q + at, part_q), part_q)
                made_q[to, :] = (old - learn_rate * got_q[pl.ds(pl.multiple_of(at, part_q), part_q), :]).astype(bf16)
                send(made_q.at[to, :], copy_q.at[to, :])
        found_o = scale * jnp.dot(left[left_o, :], table[:, cols_q:], preferred_element_type=f32)
        if mz == 0:
            moved_o[...] = found_o
            fresh_o[...] = weight_o[...] - learn_rate * found_o
            made_o[at_o, :] = fresh_o[...].astype(bf16)
            send(moved_o, step_o)
            send(fresh_o, new_o)
            send(made_o.at[at_o, :], copy_o.at[at_o, :])
        else:
            got_o[...] = found_o
            for mr in range(nr if mz == 1 else nr - 1):
                at = (r ^ mr) * part_o
                to = pl.ds(pl.multiple_of((f ^ mz) * rows_o + at, part_o), part_o)
                for k in range(cols_o // cols_q):
                    base = part_q + k * part_o
                    lo = k * cols_q
                    old = codes[mr][mz - 1, base : base + part_o, :] if mr < nr - 1 else near[base : base + part_o, :]
                    made_o[to, lo : lo + cols_q] = (
                        old - learn_rate * got_o[pl.ds(pl.multiple_of(at, part_o), part_o), lo : lo + cols_q]
                    ).astype(bf16)
                send(made_o.at[to, :], copy_o.at[to, :])
    for first, second, made_f, made_s, new_f, new_s, lo, width in (
        (first_q, second_q, made_fq, made_sq, new_fq, new_sq, 0, block_q),
        (first_o, second_o, made_fo, made_so, new_fo, new_so, block_q, block_o),
    ):
        for m in range(nr):
            cols = pl.ds(pl.multiple_of((r ^ m) * width, width), width)
            first_new, second_new, _ = moment_update(lows[m][:, lo : lo + width], first[:, cols], second[:, cols])
            made_f[:, cols] = first_new
            made_s[:, cols] = second_new
        send(made_f, new_f)
        send(made_s, new_s)
    for copy in pending:
        copy.wait()


def corner_kernel(nf, nr, place, left, table, scale, tops, ends, had_q, had_o, copy_q, copy_o, made_q, made_o, sems):
    f, r = place[0], place[1]
    scale = scale[0:1, 0:1]
    cols_q = copy_q.shape[1]
    cols_o = copy_o.shape[1]
    part_q = made_q.shape[0] // (nf - 2)
    part_o = made_o.shape[0] // (nf - 2)
    cut = nf * nr * part_q
    pending = []
    for k, mz in enumerate(range(2, nf)):
        at = (f ^ mz) * nr + (r ^ (nr - 1))
        to_q = pl.ds(pl.multiple_of(at * part_q, part_q), part_q)
        to_o = pl.ds(pl.multiple_of(at * part_o, part_o), part_o)
        got = scale * jnp.dot(left[to_q, :], table[:, 0:cols_q], preferred_element_type=f32)
        here_q = pl.ds(k * part_q, part_q)
        made_q[here_q, :] = (tops[here_q, :] - learn_rate * got).astype(bf16)
        copy = pltpu.make_async_copy(made_q.at[here_q, :], copy_q.at[to_q, :], sems.at[2 * k])
        copy.start()
        pending.append(copy)
        from_o = pl.ds(pl.multiple_of(cut + at * part_o, part_o), part_o)
        got = scale * jnp.dot(left[from_o, :], table[:, cols_q:], preferred_element_type=f32)
        here_o = pl.ds(k * part_o, part_o)
        for c in range(cols_o // cols_q):
            old = ends[pl.ds(k * part_q + c * part_o, part_o), :]
            lo = c * cols_q
            made_o[here_o, lo : lo + cols_q] = (old - learn_rate * got[:, lo : lo + cols_q]).astype(bf16)
        copy = pltpu.make_async_copy(made_o.at[here_o, :], copy_o.at[to_o, :], sems.at[2 * k + 1])
        copy.start()
        pending.append(copy)
    for copy in pending:
        copy.wait()


def shape(x, dtype=f32):
    return jax.ShapeDtypeStruct(tuple(x), dtype)


def call(kernel, outs, args, scratch=(), limit=6 * MIB, places=VMEM, source=VMEM):
    many = isinstance(outs, list)
    return pl.pallas_call(
        kernel,
        out_shape=outs,
        in_specs=[SMEM] + [source] * (len(args) - 1),
        out_specs=[places] * len(outs) if many else places,
        scratch_shapes=scratch,
        compiler_params=pltpu.CompilerParams(vmem_limit_bytes=limit),
    )(*args)


def local_short(nf, nr, inputs, query_cot, attended, output_cot, proj_query, proj_output, weight_query, weight_output, first_query, second_query, first_output, second_output):
    f, r, t = (lax.axis_index(a) for a in ("fs", "rep", "tp"))
    place = jnp.stack([f, r, t]).astype(jnp.int32)
    hold = lax.optimization_barrier

    def swap(x, axis, m, n):
        return lax.ppermute(x, axis, [(i, i ^ m) for i in range(n)])

    def batch(make, axis, n):
        got = {}
        for m in range(n - 1, 0, -1):
            got[m] = swap(make(m), axis, m, n)
        return [got[m] for m in range(1, n)]

    def over_fs(make):
        return batch(make, "fs", nf)

    def over_rep(make):
        return batch(make, "rep", nr)

    def over_tp(x):
        return swap(x, "tp", 1, 2)

    tokens = inputs.shape[0]
    rank = proj_query.shape[1]
    half = rank // 2
    rows_q, rows_o = proj_query.shape[0], proj_output.shape[0]
    part_q, part_o = rows_q // nr, rows_o // nr
    cols_q, cols_o = query_cot.shape[1], output_cot.shape[1]
    block_q, block_o = cols_q // nr, cols_o // nr
    block = block_q + block_o
    rows = rank // nf

    part = part_q + part_o
    share, both = call(
        lambda *a: share_kernel(nr, *a),
        [shape((part, half), bf16), shape((2 * part, half), bf16)],
        (place, proj_query, proj_output),
        scratch=[pltpu.SemaphoreType.DMA((6,))],
        source=ANY,
    )
    both, *far = over_fs(lambda m: both if m == 1 else share)

    def encode(at, old_q, old_o):
        parts = [lax.dynamic_slice(old_q, (at * part_q, 0), (part_q, cols_q))]
        for k in range(cols_o // cols_q):
            parts.append(lax.dynamic_slice(old_o, (at * part_o, k * cols_q), (part_o, cols_q)))
        return (jnp.concatenate(parts, axis=0) * code_scale).astype(jnp.float16)

    code = encode(r, weight_query, weight_output)
    code_far = {1: swap(code, "fs", 1, nf)}
    code_far |= {m: swap(code, "fs", m, nf) for m in range(2, nf)}

    cots = call(
        lambda *a: cot_kernel(nr, *a),
        [shape((tokens, block), bf16)] * nr,
        (place, query_cot, output_cot),
        scratch=[pltpu.SemaphoreType.DMA((2 * nr,))],
        source=ANY,
    )
    cots = [cots[0]] + over_rep(lambda m: cots[m])

    corner = call(
        lambda *a: cut_kernel(nr, *a),
        shape(code.shape),
        (place, weight_query, weight_output),
        scratch=[pltpu.SemaphoreType.DMA((1 + cols_o // cols_q,))],
        source=ANY,
    )
    corner = (corner * code_scale).astype(jnp.float16)
    corners = {1: swap(corner, "fs", 1, nf)}

    own = jnp.concatenate([both[:part], *far], axis=0)
    farther = jnp.concatenate(far, axis=0)
    near = over_rep(lambda m: own if m < nr - 1 else farther)

    table, red = call(
        lambda *a: reduce_kernel(nf, nr, *a),
        [shape(((rows_q + rows_o) * nf, half), bf16), shape((2 * half, tokens))],
        (place, inputs, attended, proj_query, proj_output, own, *near, both),
    )
    mine = [red] + over_rep(lambda m: red)
    other = [over_tp(x) for x in mine]
    parts = call(
        lambda *a: low_kernel(nf, nr, block_q, *a),
        [shape((rows, block))] * nf,
        (place, *cots, *mine, *other),
        scratch=[pltpu.VMEM((rank, block), f32)],
    )
    got = over_fs(lambda m: parts[m])

    def spread(piece):
        return swap(piece, "rep", 1, nr), swap(piece, "rep", 2, nr)

    later = hold((parts[0], *(code_far[m] for m in range(2, nf))))[1:]
    pieces = {1: code_far[1], **dict(zip(range(2, nf), later))}
    pairs = {m: spread(pieces[m]) for m in range(1, nf)}
    tops = swap(jnp.concatenate([pairs[m][0][:part_q] for m in range(2, nf)], axis=0), "rep", 2, nr)
    ends = swap(jnp.concatenate([pairs[m][1][part_q:] for m in range(2, nf)], axis=0), "rep", 1, nr)

    moments = (first_query, second_query, first_output, second_output)
    low, half_block = call(
        lambda *a: moment_kernel(nf, block_q, *a),
        [shape((rows, block)), shape((rows + TAIL, block), bf16)],
        (place, parts[0], *got, *moments),
    )
    half_far = over_fs(lambda m: half_block)
    other_table = over_tp(table)
    left = call(left_kernel, shape(((rows_q + rows_o) * nf, rank), bf16), (place, table, other_table))
    half_own, line = call(
        lambda *a: line_kernel(nf, *a), [shape((rank, block), bf16), shape((8, 128))], (place, half_block, *half_far)
    )
    halves = [half_own] + over_rep(lambda m: half_own)
    line = line + over_tp(line)
    totals = [line] + over_rep(lambda m: line)
    lows = [low] + over_rep(lambda m: low)
    near = hold((pieces[1], *pairs[1], corners[1], half_own))[:-1]
    pieces[1], pairs[1], corners[1] = near[0], near[1:3], near[3]

    def decode(x):
        return x.astype(f32) * (1.0 / code_scale)

    groups = ([pieces[m], *pairs[m]] for m in range(1, nf))
    codes = [decode(jnp.stack(x)) for x in zip(*groups)]
    count = rank * (cols_q + cols_o) * 2
    copy_q, copy_o, new_q, new_o, step_q, step_o, *new_state, all_half, scale = pl.pallas_call(
        lambda *a: step_kernel(nf, nr, block_q, count, *a),
        out_shape=[
            shape((rows_q * nf, cols_q), bf16),
            shape((rows_o * nf, cols_o), bf16),
            shape((rows_q, cols_q)),
            shape((rows_o, cols_o)),
            shape((rows_q, cols_q)),
            shape((rows_o, cols_o)),
            *[shape((rows, cols_q))] * 2,
            *[shape((rows, cols_o))] * 2,
            shape((rank, cols_q + cols_o), bf16),
            shape((8, 128)),
        ],
        in_specs=[SMEM] + [VMEM] * (4 * nr + 7),
        out_specs=[ANY] * 10 + [VMEM] * 2,
        scratch_shapes=[
            pltpu.VMEM((rows_q * nf, cols_q), bf16),
            pltpu.VMEM((rows_o * nf, cols_o), bf16),
            pltpu.VMEM((rows_q, cols_q), f32),
            pltpu.VMEM((rows_o, cols_o), f32),
            pltpu.VMEM((rows_q, cols_q), f32),
            pltpu.VMEM((rows_o, cols_o), f32),
            pltpu.VMEM((rows_q, cols_q), f32),
            pltpu.VMEM((rows_o, cols_o), f32),
            *[pltpu.VMEM((rows, cols_q), f32)] * 2,
            *[pltpu.VMEM((rows, cols_o), f32)] * 2,
            pltpu.SemaphoreType.DMA((10 + 2 * nr * (nf - 1),)),
        ],
        name="step",
        compiler_params=pltpu.CompilerParams(vmem_limit_bytes=24 * MIB),
    )(place, left, *halves, *totals, *lows, *codes, decode(corners[1]), *moments, weight_query, weight_output)
    tops, ends = hold((tops, ends, scale))[:2]
    copy_q, copy_o = pl.pallas_call(
        lambda *a: corner_kernel(nf, nr, *a),
        out_shape=[shape(copy_q.shape, bf16), shape(copy_o.shape, bf16)],
        in_specs=[SMEM] + [VMEM] * 5 + [ANY] * 2,
        out_specs=[ANY] * 2,
        scratch_shapes=[
            pltpu.VMEM(((nf - 2) * part_q, cols_q), bf16),
            pltpu.VMEM(((nf - 2) * part_o, cols_o), bf16),
            pltpu.SemaphoreType.DMA((2 * (nf - 2),)),
        ],
        input_output_aliases={6: 0, 7: 1},
        name="corner",
        compiler_params=pltpu.CompilerParams(vmem_limit_bytes=6 * MIB),
    )(place, left, all_half, scale, decode(tops), decode(ends), copy_q, copy_o)
    return (new_q, new_o, step_q, step_o, *new_state, copy_q, copy_o)


def solution(mesh):
    nf, nr, nt = (mesh.shape[a] for a in ("fs", "rep", "tp"))

    def local(*args):
        rows_o = args[5].shape[0]
        rank = args[4].shape[1]
        if nt == 2 and nf == 4 and nr == 4 and rows_o % (16 * nr) == 0 and rank % 256 == 0:
            return local_short(nf, nr, *args)
        return local_general(*args)

    spec = P("fs", "tp")
    return jax.shard_map(
        local,
        mesh=mesh,
        in_specs=(
            P(("fs", "rep"), None),
            P(("fs", "rep"), "tp"),
            P(("fs", "rep"), None),
            P(("fs", "rep"), "tp"),
            P("fs", None),
            P("fs", None),
        )
        + (spec,) * 6,
        out_specs=(spec,) * 8 + (P(None, "tp"), P(None, "tp")),
        check_vma=False,
    )
```

```python
import jax
import jax.numpy as jnp
from jax import lax
from jax.experimental import pallas as pl
from jax.experimental.pallas import tpu as pltpu
from jax.sharding import PartitionSpec as P

beta_first = 0.9
beta_second = 0.95
adam_eps = 1e-08
mean_eps = 1e-06
learn_rate = 0.02
code_scale = 2.0**17


f32 = jnp.float32
bf16 = jnp.bfloat16
VMEM = pl.BlockSpec(memory_space=pltpu.VMEM)
SMEM = pl.BlockSpec(memory_space=pltpu.SMEM)
ANY = pl.BlockSpec(memory_space=pl.ANY)
HBM = pl.BlockSpec(memory_space=pltpu.HBM)
TAIL = 16
MIB = 2**20


def moment_update(low_sum, first, second):
    first_new = beta_first * first + (1.0 - beta_first) * low_sum
    second_new = beta_second * second + (1.0 - beta_second) * low_sum * low_sum
    normed = first_new / (jnp.sqrt(second_new) + adam_eps)
    return (first_new, second_new, normed)


def contract_rows(left, right):
    return lax.dot_general(
        left,
        right,
        (((0,), (0,)), ((), ())),
        precision=lax.Precision.HIGHEST,
        preferred_element_type=f32,
    )


def local_general(inputs, query_cot, attended, output_cot, proj_query, proj_output, weight_query, weight_output, first_query, second_query, first_output, second_output):
    def gather(x):
        return lax.all_gather(x, "fs", axis=0, tiled=True)

    def low_of(acts, proj, cot):
        reduced = jnp.dot(acts, gather(proj), preferred_element_type=f32)
        part = contract_rows(reduced, cot.astype(f32))
        return lax.psum_scatter(part, "fs", scatter_dimension=0, tiled=True)

    low_query, low_output = lax.psum((low_of(inputs, proj_query, query_cot), low_of(attended, proj_output, output_cot)), "rep")
    first_q, second_q, normed_q = moment_update(low_query, first_query, second_query)
    first_o, second_o, normed_o = moment_update(low_output, first_output, second_output)
    total = lax.psum(jnp.sum(normed_q * normed_q) + jnp.sum(normed_o * normed_o), ("fs", "tp"))
    entries = (normed_q.size + normed_o.size) * lax.axis_size("fs") * lax.axis_size("tp")
    scale = lax.rsqrt(total / entries + mean_eps)
    step_q = scale * jnp.dot(proj_query, gather(normed_q.astype(bf16)), preferred_element_type=f32)
    step_o = scale * jnp.dot(proj_output, gather(normed_o.astype(bf16)), preferred_element_type=f32)
    new_q = weight_query - learn_rate * step_q
    new_o = weight_output - learn_rate * step_o
    return (new_q, new_o, step_q, step_o, first_q, second_q, first_o, second_o, gather(new_q.astype(bf16)), gather(new_o.astype(bf16)))


def fetch(pairs, sems):
    copies = [pltpu.make_async_copy(src, dst, sems.at[k]) for k, (src, dst) in enumerate(pairs)]
    for copy in copies:
        copy.start()
    for copy in copies:
        copy.wait()


def share_kernel(nr, place, proj_q, proj_o, share, both, sems):
    r, t = place[1], place[2]
    part_q, part_o, half = proj_q.shape[0] // nr, proj_o.shape[0] // nr, share.shape[1]
    part = part_q + part_o
    mine = pl.ds(pl.multiple_of(t * half, half), half)
    pairs = []
    for at, out, base in ((r, share, 0), (r, both, 0), (r ^ (nr - 1), both, part)):
        pairs.append((proj_q.at[pl.ds(pl.multiple_of(at * part_q, part_q), part_q), mine], out.at[base : base + part_q, :]))
        pairs.append((proj_o.at[pl.ds(pl.multiple_of(at * part_o, part_o), part_o), mine], out.at[base + part_q : base + part, :]))
    fetch(pairs, sems)


def cot_kernel(nr, place, cot_q, cot_o, *rest):
    outs, sems = rest[:-1], rest[-1]
    r = place[1]
    block_q, block_o = cot_q.shape[1] // nr, cot_o.shape[1] // nr
    pairs = []
    for m, out in enumerate(outs):
        at = r ^ m
        pairs.append((cot_q.at[:, pl.ds(pl.multiple_of(at * block_q, block_q), block_q)], out.at[:, 0:block_q]))
        pairs.append((cot_o.at[:, pl.ds(pl.multiple_of(at * block_o, block_o), block_o)], out.at[:, block_q : block_q + block_o]))
    fetch(pairs, sems)


def cut_kernel(nr, place, weight_q, weight_o, out, sems):
    at = place[1] ^ (nr - 1)
    part_q, part_o = weight_q.shape[0] // nr, weight_o.shape[0] // nr
    cols = weight_q.shape[1]
    pairs = [(weight_q.at[pl.ds(pl.multiple_of(at * part_q, part_q), part_q), :], out.at[0:part_q, :])]
    for k in range(weight_o.shape[1] // cols):
        base = part_q + k * part_o
        rows = pl.ds(pl.multiple_of(at * part_o, part_o), part_o)
        pairs.append((weight_o.at[rows, k * cols : (k + 1) * cols], out.at[base : base + part_o, :]))
    fetch(pairs, sems)


def reduce_kernel(nf, nr, place, inputs, attended, proj_q, proj_o, own, *rest):
    near, (both, table, red) = rest[:-3], rest[-3:]
    f, r, t = place[0], place[1], place[2]
    half = table.shape[1]
    rows_q, rows_o = proj_q.shape[0], proj_o.shape[0]
    part_q, part_o = rows_q // nr, rows_o // nr
    part = part_q + part_o
    cut = nf * rows_q
    mine = pl.ds(pl.multiple_of(t * half, half), half)
    table[pl.ds(pl.multiple_of(f * rows_q, rows_q), rows_q), :] = proj_q[:, mine]
    table[pl.ds(pl.multiple_of(cut + f * rows_o, rows_o), rows_o), :] = proj_o[:, mine]
    for mr, whole in enumerate((own,) + near):
        for mz in range(1, nf):
            at = (f ^ mz) * nr + (r ^ mr)
            ref, base = whole, (mz - 1) * part
            if mr == nr - 1:
                ref, base = (both, part) if mz == 1 else (whole, base - part)
            table[pl.ds(pl.multiple_of(at * part_q, part_q), part_q), :] = ref[base : base + part_q, :]
            table[pl.ds(pl.multiple_of(cut + at * part_o, part_o), part_o), :] = ref[base + part_q : base + part, :]
    red_q = jnp.dot(inputs[...], table[0:cut, :], preferred_element_type=f32)
    red_o = jnp.dot(attended[...], table[cut:, :], preferred_element_type=f32)
    red[0:half, :] = red_q.T
    red[half : 2 * half, :] = red_o.T


def split_three(x):
    high = x.astype(bf16)
    rest = x - high.astype(f32)
    mid = rest.astype(bf16)
    return high, mid, (rest - mid.astype(f32)).astype(bf16)


def low_kernel(nf, nr, block_q, place, *refs):
    cots, mine, other, outs, low = refs[:nr], refs[nr : 2 * nr], refs[2 * nr : 3 * nr], refs[3 * nr : 3 * nr + nf], refs[-1]
    f, t = place[0], place[2]
    half = mine[0].shape[0] // 2
    cot = jnp.concatenate([c[...] for c in cots], axis=0)
    for which, group in enumerate((mine, other)):
        top = pl.multiple_of((t ^ which) * half, half)
        for k, (lo, hi) in enumerate(((0, block_q), (block_q, cot.shape[1]))):
            left = jnp.concatenate([g[k * half : (k + 1) * half, :] for g in group], axis=1)
            acc = None
            for term in split_three(left):
                got = jnp.dot(term, cot[:, lo:hi], preferred_element_type=f32)
                acc = got if acc is None else acc + got
            low[pl.ds(top, half), lo:hi] = acc
    rows = low.shape[0] // nf
    for m in range(nf):
        outs[m][...] = low[pl.ds(pl.multiple_of((f ^ m) * rows, rows), rows), :]


def pack_total(spread):
    row = lax.broadcasted_iota(jnp.int32, spread.shape, 0)
    high, mid, last = (x.astype(f32) for x in split_three(spread))
    packed = jnp.where(row == 0, high, jnp.where(row == 1, mid, jnp.where(row == 2, last, 0.0)))
    return jnp.concatenate([packed, jnp.zeros_like(packed)], axis=0).astype(bf16)


def pairwise(terms):
    while len(terms) > 1:
        terms = [a + b for a, b in zip(terms[::2], terms[1::2])]
    return terms[0]


def add_totals(tails):
    return jnp.sum(pairwise([tail.astype(f32) for tail in tails]), axis=0, keepdims=True)


def moment_kernel(nf, block_q, place, *refs):
    parts, (first_q, second_q, first_o, second_o, low_out, half_out) = refs[:nf], refs[nf:]
    r = place[1]
    low = parts[0][...]
    for p in parts[1:]:
        low = low + p[...]
    low_out[...] = low
    block_o = low.shape[1] - block_q
    rows = low.shape[0]
    total = jnp.zeros((), f32)
    for first, second, lo, width in ((first_q, second_q, 0, block_q), (first_o, second_o, block_q, block_o)):
        cols = pl.ds(pl.multiple_of(r * width, width), width)
        _, _, normed = moment_update(low[:, lo : lo + width], first[:, cols], second[:, cols])
        half_out[0:rows, lo : lo + width] = normed.astype(bf16)
        total = total + jnp.sum(normed * normed)
    half_out[rows : rows + TAIL, :] = pack_total(jnp.full((8, low.shape[1]), total, f32))


def line_kernel(nf, place, *refs):
    blocks, (table, total) = refs[:nf], refs[nf:]
    f = place[0]
    rows = blocks[0].shape[0] - TAIL
    for m, block in enumerate(blocks):
        table[pl.ds(pl.multiple_of((f ^ m) * rows, rows), rows), :] = block[0:rows, :]
    found = add_totals([block[rows : rows + TAIL, 0 : total.shape[1]] for block in blocks])
    total[...] = jnp.broadcast_to(found, total.shape)


def left_kernel(place, mine, other, out):
    t = place[2]
    half = mine.shape[1]
    out[:, pl.ds(pl.multiple_of(t * half, half), half)] = mine[...]
    out[:, pl.ds(pl.multiple_of((1 - t) * half, half), half)] = other[...]


def step_kernel(nf, nr, block_q, count, place, left, *rest):
    halves, totals, lows, rest = rest[:nr], rest[nr : 2 * nr], rest[2 * nr : 3 * nr], rest[3 * nr :]
    codes, near, rest = rest[: nr - 1], rest[nr - 1], rest[nr:]
    first_q, second_q, first_o, second_o, weight_q, weight_o, sent_q, sent_o = rest[:8]
    copy_q, copy_o, new_q, new_o, step_q, step_o, new_fq, new_sq, new_fo, new_so, table, scale_out = rest[8:20]
    made_q, made_o, fresh_q, fresh_o, moved_q, moved_o, got_q, got_o, made_fq, made_sq, made_fo, made_so, sems = rest[20:]
    f, r = place[0], place[1]
    rows_q, cols_q = weight_q.shape
    rows_o, cols_o = weight_o.shape
    part_q, part_o = rows_q // nr, rows_o // nr
    cut = nf * rows_q
    block_o = cols_o // nr
    total = pairwise([x[...] for x in totals])
    scale = lax.rsqrt(total / count + mean_eps)
    scale_out[...] = scale
    scale = scale[0:1, 0:1]

    for m in range(nr):
        at = r ^ m
        table[:, pl.ds(pl.multiple_of(at * block_q, block_q), block_q)] = halves[m][:, 0:block_q]
        table[:, pl.ds(pl.multiple_of(cols_q + at * block_o, block_o), block_o)] = halves[m][:, block_q:]

    pending = []

    def send(src, dst):
        copy = pltpu.make_async_copy(src, dst, sems.at[len(pending)])
        copy.start()
        pending.append(copy)

    for mz in range(nf):
        at_q = pl.ds(pl.multiple_of((f ^ mz) * rows_q, rows_q), rows_q)
        at_o = pl.ds(pl.multiple_of((f ^ mz) * rows_o, rows_o), rows_o)
        left_o = pl.ds(pl.multiple_of(cut + (f ^ mz) * rows_o, rows_o), rows_o)
        found_q = scale * jnp.dot(left[at_q, :], table[:, 0:cols_q], preferred_element_type=f32)
        if mz == 0:
            moved_q[...] = found_q
            fresh_q[...] = weight_q[...] - learn_rate * found_q
            made_q[at_q, :] = (sent_q[...] - learn_rate * found_q).astype(bf16)
            send(moved_q, step_q)
            send(fresh_q, new_q)
            send(made_q.at[at_q, :], copy_q.at[at_q, :])
        else:
            got_q[...] = found_q
            for mr in range(nr if mz == 1 else nr - 1):
                at = (r ^ mr) * part_q
                old = codes[mr][mz - 1, 0:part_q, :] if mr < nr - 1 else near[0:part_q, :]
                to = pl.ds(pl.multiple_of((f ^ mz) * rows_q + at, part_q), part_q)
                made_q[to, :] = (old - learn_rate * got_q[pl.ds(pl.multiple_of(at, part_q), part_q), :]).astype(bf16)
                send(made_q.at[to, :], copy_q.at[to, :])
        found_o = scale * jnp.dot(left[left_o, :], table[:, cols_q:], preferred_element_type=f32)
        if mz == 0:
            moved_o[...] = found_o
            fresh_o[...] = weight_o[...] - learn_rate * found_o
            made_o[at_o, :] = (sent_o[...] - learn_rate * found_o).astype(bf16)
            send(moved_o, step_o)
            send(fresh_o, new_o)
            send(made_o.at[at_o, :], copy_o.at[at_o, :])
        else:
            got_o[...] = found_o
            for mr in range(nr if mz == 1 else nr - 1):
                at = (r ^ mr) * part_o
                to = pl.ds(pl.multiple_of((f ^ mz) * rows_o + at, part_o), part_o)
                for k in range(cols_o // cols_q):
                    base = part_q + k * part_o
                    lo = k * cols_q
                    old = codes[mr][mz - 1, base : base + part_o, :] if mr < nr - 1 else near[base : base + part_o, :]
                    made_o[to, lo : lo + cols_q] = (
                        old - learn_rate * got_o[pl.ds(pl.multiple_of(at, part_o), part_o), lo : lo + cols_q]
                    ).astype(bf16)
                send(made_o.at[to, :], copy_o.at[to, :])
    for first, second, made_f, made_s, new_f, new_s, lo, width in (
        (first_q, second_q, made_fq, made_sq, new_fq, new_sq, 0, block_q),
        (first_o, second_o, made_fo, made_so, new_fo, new_so, block_q, block_o),
    ):
        for m in range(nr):
            cols = pl.ds(pl.multiple_of((r ^ m) * width, width), width)
            first_new, second_new, _ = moment_update(lows[m][:, lo : lo + width], first[:, cols], second[:, cols])
            made_f[:, cols] = first_new
            made_s[:, cols] = second_new
        send(made_f, new_f)
        send(made_s, new_s)
    for copy in pending:
        copy.wait()


def corner_kernel(nf, nr, place, left, table, scale, tops, ends, had_q, had_o, copy_q, copy_o, made_q, made_o, sems):
    f, r = place[0], place[1]
    scale = scale[0:1, 0:1]
    cols_q = copy_q.shape[1]
    cols_o = copy_o.shape[1]
    part_q = made_q.shape[0] // (nf - 2)
    part_o = made_o.shape[0] // (nf - 2)
    cut = nf * nr * part_q
    pending = []
    for k, mz in enumerate(range(2, nf)):
        at = (f ^ mz) * nr + (r ^ (nr - 1))
        to_q = pl.ds(pl.multiple_of(at * part_q, part_q), part_q)
        to_o = pl.ds(pl.multiple_of(at * part_o, part_o), part_o)
        got = scale * jnp.dot(left[to_q, :], table[:, 0:cols_q], preferred_element_type=f32)
        here_q = pl.ds(k * part_q, part_q)
        made_q[here_q, :] = (tops[here_q, :] - learn_rate * got).astype(bf16)
        copy = pltpu.make_async_copy(made_q.at[here_q, :], copy_q.at[to_q, :], sems.at[2 * k])
        copy.start()
        pending.append(copy)
        from_o = pl.ds(pl.multiple_of(cut + at * part_o, part_o), part_o)
        got = scale * jnp.dot(left[from_o, :], table[:, cols_q:], preferred_element_type=f32)
        here_o = pl.ds(k * part_o, part_o)
        for c in range(cols_o // cols_q):
            old = ends[pl.ds(k * part_q + c * part_o, part_o), :]
            lo = c * cols_q
            made_o[here_o, lo : lo + cols_q] = (old - learn_rate * got[:, lo : lo + cols_q]).astype(bf16)
        copy = pltpu.make_async_copy(made_o.at[here_o, :], copy_o.at[to_o, :], sems.at[2 * k + 1])
        copy.start()
        pending.append(copy)
    for copy in pending:
        copy.wait()


def shape(x, dtype=f32):
    return jax.ShapeDtypeStruct(tuple(x), dtype)


def call(kernel, outs, args, scratch=(), limit=6 * MIB, places=VMEM, source=VMEM):
    many = isinstance(outs, list)
    return pl.pallas_call(
        kernel,
        out_shape=outs,
        in_specs=[SMEM] + [source] * (len(args) - 1),
        out_specs=[places] * len(outs) if many else places,
        scratch_shapes=scratch,
        compiler_params=pltpu.CompilerParams(vmem_limit_bytes=limit),
    )(*args)


def local_short(nf, nr, inputs, query_cot, attended, output_cot, proj_query, proj_output, weight_query, weight_output, first_query, second_query, first_output, second_output):
    f, r, t = (lax.axis_index(a) for a in ("fs", "rep", "tp"))
    place = jnp.stack([f, r, t]).astype(jnp.int32)
    hold = lax.optimization_barrier

    def swap(x, axis, m, n):
        return lax.ppermute(x, axis, [(i, i ^ m) for i in range(n)])

    def batch(make, axis, n):
        got = {}
        for m in range(n - 1, 0, -1):
            got[m] = swap(make(m), axis, m, n)
        return [got[m] for m in range(1, n)]

    def over_fs(make):
        return batch(make, "fs", nf)

    def over_rep(make):
        return batch(make, "rep", nr)

    def over_tp(x):
        return swap(x, "tp", 1, 2)

    tokens = inputs.shape[0]
    rank = proj_query.shape[1]
    half = rank // 2
    rows_q, rows_o = proj_query.shape[0], proj_output.shape[0]
    part_q, part_o = rows_q // nr, rows_o // nr
    cols_q, cols_o = query_cot.shape[1], output_cot.shape[1]
    block_q, block_o = cols_q // nr, cols_o // nr
    block = block_q + block_o
    rows = rank // nf

    part = part_q + part_o
    share, both = call(
        lambda *a: share_kernel(nr, *a),
        [shape((part, half), bf16), shape((2 * part, half), bf16)],
        (place, proj_query, proj_output),
        scratch=[pltpu.SemaphoreType.DMA((6,))],
        source=ANY,
    )
    both, *far = over_fs(lambda m: both if m == 1 else share)

    def encode(at, old_q, old_o):
        parts = [lax.dynamic_slice(old_q, (at * part_q, 0), (part_q, cols_q))]
        for k in range(cols_o // cols_q):
            parts.append(lax.dynamic_slice(old_o, (at * part_o, k * cols_q), (part_o, cols_q)))
        return (jnp.concatenate(parts, axis=0) * code_scale).astype(jnp.float16)

    code = encode(r, weight_query, weight_output)
    code_far = {1: swap(code, "fs", 1, nf)}
    code_far |= {m: swap(code, "fs", m, nf) for m in range(2, nf)}

    sent = [lax.reduce_precision(x * code_scale, 5, 10) * (1.0 / code_scale) for x in (weight_query, weight_output)]

    cots = call(
        lambda *a: cot_kernel(nr, *a),
        [shape((tokens, block), bf16)] * nr,
        (place, query_cot, output_cot),
        scratch=[pltpu.SemaphoreType.DMA((2 * nr,))],
        source=ANY,
    )
    cots = [cots[0]] + over_rep(lambda m: cots[m])

    corner = call(
        lambda *a: cut_kernel(nr, *a),
        shape(code.shape),
        (place, weight_query, weight_output),
        scratch=[pltpu.SemaphoreType.DMA((1 + cols_o // cols_q,))],
        source=ANY,
    )
    corner = (corner * code_scale).astype(jnp.float16)
    corners = {1: swap(corner, "fs", 1, nf)}

    own = jnp.concatenate([both[:part], *far], axis=0)
    farther = jnp.concatenate(far, axis=0)
    near = over_rep(lambda m: own if m < nr - 1 else farther)

    table, red = call(
        lambda *a: reduce_kernel(nf, nr, *a),
        [shape(((rows_q + rows_o) * nf, half), bf16), shape((2 * half, tokens))],
        (place, inputs, attended, proj_query, proj_output, own, *near, both),
    )
    mine = [red] + over_rep(lambda m: red)
    other = [over_tp(x) for x in mine]
    parts = call(
        lambda *a: low_kernel(nf, nr, block_q, *a),
        [shape((rows, block))] * nf,
        (place, *cots, *mine, *other),
        scratch=[pltpu.VMEM((rank, block), f32)],
    )
    got = over_fs(lambda m: parts[m])

    def spread(piece):
        return swap(piece, "rep", 1, nr), swap(piece, "rep", 2, nr)

    later = hold((parts[0], *(code_far[m] for m in range(2, nf))))[1:]
    pieces = {1: code_far[1], **dict(zip(range(2, nf), later))}
    pairs = {m: spread(pieces[m]) for m in range(1, nf)}
    tops = swap(jnp.concatenate([pairs[m][0][:part_q] for m in range(2, nf)], axis=0), "rep", 2, nr)
    ends = swap(jnp.concatenate([pairs[m][1][part_q:] for m in range(2, nf)], axis=0), "rep", 1, nr)

    moments = (first_query, second_query, first_output, second_output)
    low, half_block = call(
        lambda *a: moment_kernel(nf, block_q, *a),
        [shape((rows, block)), shape((rows + TAIL, block), bf16)],
        (place, parts[0], *got, *moments),
    )
    half_far = over_fs(lambda m: half_block)
    other_table = over_tp(table)
    left = call(left_kernel, shape(((rows_q + rows_o) * nf, rank), bf16), (place, table, other_table))
    half_own, line = call(
        lambda *a: line_kernel(nf, *a), [shape((rank, block), bf16), shape((8, 128))], (place, half_block, *half_far)
    )
    halves = [half_own] + over_rep(lambda m: half_own)
    line = line + over_tp(line)
    totals = [line] + over_rep(lambda m: line)
    lows = [low] + over_rep(lambda m: low)
    near = hold((pieces[1], *pairs[1], corners[1], half_own))[:-1]
    pieces[1], pairs[1], corners[1] = near[0], near[1:3], near[3]

    def decode(x):
        return x.astype(f32) * (1.0 / code_scale)

    groups = ([pieces[m], *pairs[m]] for m in range(1, nf))
    codes = [decode(jnp.stack(x)) for x in zip(*groups)]
    count = rank * (cols_q + cols_o) * 2
    copy_q, copy_o, new_q, new_o, step_q, step_o, *new_state, all_half, scale = pl.pallas_call(
        lambda *a: step_kernel(nf, nr, block_q, count, *a),
        out_shape=[
            shape((rows_q * nf, cols_q), bf16),
            shape((rows_o * nf, cols_o), bf16),
            shape((rows_q, cols_q)),
            shape((rows_o, cols_o)),
            shape((rows_q, cols_q)),
            shape((rows_o, cols_o)),
            *[shape((rows, cols_q))] * 2,
            *[shape((rows, cols_o))] * 2,
            shape((rank, cols_q + cols_o), bf16),
            shape((8, 128)),
        ],
        in_specs=[SMEM] + [VMEM] * (4 * nr + 9),
        out_specs=[ANY] * 10 + [VMEM] * 2,
        scratch_shapes=[
            pltpu.VMEM((rows_q * nf, cols_q), bf16),
            pltpu.VMEM((rows_o * nf, cols_o), bf16),
            pltpu.VMEM((rows_q, cols_q), f32),
            pltpu.VMEM((rows_o, cols_o), f32),
            pltpu.VMEM((rows_q, cols_q), f32),
            pltpu.VMEM((rows_o, cols_o), f32),
            pltpu.VMEM((rows_q, cols_q), f32),
            pltpu.VMEM((rows_o, cols_o), f32),
            *[pltpu.VMEM((rows, cols_q), f32)] * 2,
            *[pltpu.VMEM((rows, cols_o), f32)] * 2,
            pltpu.SemaphoreType.DMA((10 + 2 * nr * (nf - 1),)),
        ],
        name="step",
        compiler_params=pltpu.CompilerParams(vmem_limit_bytes=24 * MIB),
    )(place, left, *halves, *totals, *lows, *codes, decode(corners[1]), *moments, weight_query, weight_output, *sent)
    tops, ends = hold((tops, ends, scale))[:2]
    copy_q, copy_o = pl.pallas_call(
        lambda *a: corner_kernel(nf, nr, *a),
        out_shape=[shape(copy_q.shape, bf16), shape(copy_o.shape, bf16)],
        in_specs=[SMEM] + [VMEM] * 5 + [ANY] * 2,
        out_specs=[ANY] * 2,
        scratch_shapes=[
            pltpu.VMEM(((nf - 2) * part_q, cols_q), bf16),
            pltpu.VMEM(((nf - 2) * part_o, cols_o), bf16),
            pltpu.SemaphoreType.DMA((2 * (nf - 2),)),
        ],
        input_output_aliases={6: 0, 7: 1},
        name="corner",
        compiler_params=pltpu.CompilerParams(vmem_limit_bytes=6 * MIB),
    )(place, left, all_half, scale, decode(tops), decode(ends), copy_q, copy_o)
    return (new_q, new_o, step_q, step_o, *new_state, copy_q, copy_o)


def solution(mesh):
    nf, nr, nt = (mesh.shape[a] for a in ("fs", "rep", "tp"))

    def local(*args):
        rows_o = args[5].shape[0]
        rank = args[4].shape[1]
        if nt == 2 and nf == 4 and nr == 4 and rows_o % (16 * nr) == 0 and rank % 256 == 0:
            return local_short(nf, nr, *args)
        return local_general(*args)

    spec = P("fs", "tp")
    return jax.shard_map(
        local,
        mesh=mesh,
        in_specs=(
            P(("fs", "rep"), None),
            P(("fs", "rep"), "tp"),
            P(("fs", "rep"), None),
            P(("fs", "rep"), "tp"),
            P("fs", None),
            P("fs", None),
        )
        + (spec,) * 6,
        out_specs=(spec,) * 8 + (P(None, "tp"), P(None, "tp")),
        check_vma=False,
    )
```
